32 devices in a mesh: kv: 16 (over z, x, core), tp: 2 (over y).
Axes of the slice: x: 2, y: 2, z: 4, core: 2. Of those that a mesh axis runs over, the one named last changes fastest.
Arguments:
- hidden_in: bfloat16 [4, 1024, 2048], P(None, 'kv'), may hold values from -84 to 84
- w_query: bfloat16 [2048, 1024], P(None, 'tp'), may hold values from -0.125 to 0.125
- w_cmp_key: bfloat16 [2048, 256], P(None, 'tp'), may hold values from -0.125 to 0.125
- w_cmp_value: bfloat16 [2048, 256], P(None, 'tp'), may hold values from -0.8838835 to 0.8838835
- w_sel_key: bfloat16 [2048, 256], P(None, 'tp'), may hold values from -0.125 to 0.125
- w_sel_value: bfloat16 [2048, 256], P(None, 'tp'), may hold values from -0.8838835 to 0.8838835
- w_gate: bfloat16 [2048, 2, 16], replicated, may hold values from -0.125 to 0.125
- cmp_key_in: bfloat16 [2048, 128], replicated, may hold values from -0.125 to 0.125
- cmp_key_out: bfloat16 [128, 64], replicated, may hold values from -0.5 to 0.5
- cmp_value_in: bfloat16 [2048, 128], replicated, may hold values from -0.125 to 0.125
- cmp_value_out: bfloat16 [128, 64], replicated, may hold values from -0.5 to 0.5
- out_gain: float32 [1024], replicated, may hold values from 0.1 to 1.9
- w_out: bfloat16 [1024, 2048], replicated, may hold values from -0.1875 to 0.1875
- seq_lengths: int32 [4], replicated, may hold values from 1 to 1024, 1638 in all
- chosen: int32 [4, 16, 4, 16], P(None, 'kv', 'tp'), may hold values from -1 to 15, as said below
Outputs:
- attended: bfloat16 [4, 1024, 2048], P(None, 'kv', 'tp')
The draws below stay inside these ranges and needn't reach their ends.
Inputs may be any that keep to these rules, and one draw needn't show every extreme that they name: chosen[s, b, g, 0] is b itself. Every other entry is -1 or a block index below b, and the entries of one list that are not -1 are distinct. For each block index and key group, the entries after the first slot that name that index all lie in the lists of a single sequence.
All inputs are finite; a program needn't handle non-finite values.
Results may differ from the reference program's by a relative error of at most 0.012.
The reference program's roundings to bfloat16 on the way count: a program that leaves them out, or rounds other values in their place, can miss the bound.
Values may be sent and summed in bfloat16 or wider, within the bound.
A program may use at most 64 MiB of HBM per device.

```python
import math
import jax
import jax.numpy as jnp
import numpy as np
from jax import lax

D = 2048
HEADS = 16
GROUPS = 4
HEAD_DIM = 64
CMP_STRIDE = 16
CMP_BLOCK = 32
CMP_HIDDEN = 128
SLC_BLOCK = 64
TOPK = 16
SEQS = 4
SEQ_LEN = 1024
BLOCKS = 16


def rising_columns(key):
    base = jnp.clip(jax.random.normal(key, (D, GROUPS * HEAD_DIM), jnp.float32), -4.0, 4.0) * D ** (-0.5)
    group = (jnp.arange(GROUPS * HEAD_DIM) // HEAD_DIM).astype(jnp.float32)
    factor = 3.0 ** (group / (GROUPS - 1))
    return (base * factor[None, :]).astype(jnp.bfloat16)


def draw_w_cmp_value(key, part):
    return rising_columns(jax.random.fold_in(key, 31))


def draw_w_sel_value(key, part):
    return rising_columns(jax.random.fold_in(key, 32))


def draw_hidden_in(key, part):
    shape = (SEQS, SEQ_LEN, D)
    base = jnp.clip(jax.random.normal(jax.random.fold_in(key, 41), shape, jnp.float32), -6.0, 6.0)
    return base.astype(jnp.bfloat16)


def draw_chosen(key, part):
    block_list = SEQ_LEN // SLC_BLOCK
    owner_seq = jax.random.randint(jax.random.fold_in(key, 51), (block_list, GROUPS), 0, SEQS)
    heat = jax.random.randint(jax.random.fold_in(key, 52), (block_list,), 0, 4)
    random_jitter = jax.random.randint(jax.random.fold_in(key, 53), (SEQS, block_list, GROUPS, block_list), 0, 4096)
    local_block = jnp.arange(block_list)[None, :, None, None]
    remote_block = jnp.arange(block_list)[None, None, None, :]
    seq_ids = jnp.arange(SEQS)[:, None, None, None]
    owner = jnp.transpose(owner_seq)[None, None, :, :]
    valid = (remote_block < local_block) & (owner == seq_ids)
    closest_block = jnp.max(jnp.where(valid, remote_block, -1), axis=-1, keepdims=True)
    extra_score = jnp.where(remote_block == closest_block, 1 << 20, 0) + jnp.where(remote_block == local_block - block_list // 2, 1 << 19, 0)
    weight_matrix = heat * heat * 4096
    block_score = (weight_matrix[None, None, None, :] + random_jitter + extra_score) * block_list + remote_block
    block_score = jnp.where(valid, block_score, -1 - remote_block)
    values, indices = lax.top_k(block_score, TOPK - 1)
    picked = jnp.where(values >= 0, indices, -1)
    own = jnp.broadcast_to(local_block, (SEQS, block_list, GROUPS, 1))
    return jnp.concatenate([own, picked], axis=-1).astype(jnp.int32)


def levels(rng, extent, pieces, low, top_value):
    def one(axis_at, blocks):
        draws = jax.random.uniform(jax.random.fold_in(jax.random.fold_in(rng, 6), axis_at), (blocks,), jnp.float32, low / len(pieces), top_value / len(pieces))
        return jnp.repeat(jnp.exp(draws), extent[axis_at] // blocks).reshape((-1,) + (1,) * (len(extent) - axis_at - 1))

    factor_of = one(*pieces[0])
    for cut in pieces[1:]:
        factor_of = factor_of * one(*cut)
    return factor_of


def length_profile(amount, total, limit, skew):
    loads = [(1 << 20) // math.isqrt(rank ** skew) + 1 for rank in range(2, amount + 1)]
    rest, holding = total - limit - (amount - 1), [1] * (amount - 1)
    while rest > 0:
        movable = [i for i in range(amount - 1) if holding[i] < limit]
        pool, left = sum([loads[i] for i in movable]), rest
        for i in movable:
            addition = min(limit - holding[i], max(1, left * loads[i] // pool), rest)
            holding[i] = holding[i] + addition
            rest = rest - addition
    return np.array([limit] + holding)


def ragged(own_key, amount, total, limit, slope):
    if amount == 2:
        one = jax.random.randint(own_key, (), max(1, total - limit), min(limit, total - 1) + 1)
        return jnp.stack([one, total - one])
    lengths = jnp.asarray(length_profile(amount, total, limit, slope), jnp.int32)
    couples = (amount - 1) // 2
    donor, taker = lengths[1:1 + 2 * couples:2], lengths[2:2 + 2 * couples:2]
    margin = jnp.minimum(donor - 1, limit - taker)
    moved = jax.random.randint(jax.random.fold_in(own_key, 1), (couples,), 0, 1 << 20) % (margin + 1)
    lengths = lengths.at[1:1 + 2 * couples:2].set(donor - moved).at[2:2 + 2 * couples:2].set(taker + moved)
    return lengths[jax.random.permutation(jax.random.fold_in(own_key, 2), amount)]


def normal_values(own_key, extent, deviation, most, shards=(), kind=jnp.bfloat16):
    values = jax.random.normal(own_key, extent, jnp.float32) * deviation
    if len(shards) > 0:
        values = levels(own_key, extent, shards, -0.22, 0.18) * values
    return jnp.clip(values, min=-most, max=most).astype(kind)


def setup_inputs(seed: int = 0) -> dict:
    splits = jax.random.split(jax.random.key(seed), 16)
    hidden_in = draw_hidden_in(jax.random.fold_in(splits[15], 71), 0)
    w_query = normal_values(splits[1], (D, HEADS * HEAD_DIM), D ** -0.5, 0.125, ((1, 2),))
    w_cmp_key = normal_values(splits[2], (D, GROUPS * HEAD_DIM), D ** -0.5, 0.125, ((1, 2),))
    w_cmp_value = draw_w_cmp_value(jax.random.fold_in(splits[15], 71), 0)
    w_sel_key = normal_values(splits[4], (D, GROUPS * HEAD_DIM), D ** -0.5, 0.125, ((1, 2),))
    w_sel_value = draw_w_sel_value(jax.random.fold_in(splits[15], 71), 0)
    w_gate = normal_values(splits[6], (D, 2, HEADS), D ** -0.5, 0.125)
    cmp_key_in = normal_values(splits[7], (CMP_BLOCK * HEAD_DIM, CMP_HIDDEN), (CMP_BLOCK * HEAD_DIM) ** -0.5, 0.125)
    cmp_key_out = normal_values(splits[8], (CMP_HIDDEN, HEAD_DIM), CMP_HIDDEN ** -0.5, 0.5)
    cmp_value_in = normal_values(splits[9], (CMP_BLOCK * HEAD_DIM, CMP_HIDDEN), (CMP_BLOCK * HEAD_DIM) ** -0.5, 0.125)
    cmp_value_out = normal_values(splits[10], (CMP_HIDDEN, HEAD_DIM), CMP_HIDDEN ** -0.5, 0.5)
    out_gain = jnp.clip(1.0 + 0.18 * jax.random.normal(splits[11], (HEADS * HEAD_DIM,), jnp.float32), 0.1, 1.9)
    w_out = normal_values(splits[12], (HEADS * HEAD_DIM, D), (HEADS * HEAD_DIM) ** -0.5, 0.1875)
    seq_lengths = ragged(splits[13], SEQS, SEQ_LEN + (SEQS - 1) * SEQ_LEN // 5, SEQ_LEN, 2).astype(jnp.int32)
    chosen = draw_chosen(jax.random.fold_in(splits[15], 71), 0)
    return {"hidden_in": hidden_in, "w_query": w_query, "w_cmp_key": w_cmp_key, "w_cmp_value": w_cmp_value, "w_sel_key": w_sel_key, "w_sel_value": w_sel_value, "w_gate": w_gate, "cmp_key_in": cmp_key_in, "cmp_key_out": cmp_key_out, "cmp_value_in": cmp_value_in, "cmp_value_out": cmp_value_out, "out_gain": out_gain, "w_out": w_out, "seq_lengths": seq_lengths, "chosen": chosen}


theta_base = 500000.0
norm_eps = 1e-06

def rotate(values, positions):
    width = values.shape[-1]
    half = width // 2
    inverse = jnp.exp(-jnp.log(jnp.float32(theta_base)) * jnp.arange(0, width, 2).astype(jnp.float32) / width)
    angle = positions.astype(jnp.float32)[:, None] * inverse[None, :]
    cosine = jnp.cos(angle)[:, None, :]
    sine = jnp.sin(angle)[:, None, :]
    first = values[..., :half]
    second = values[..., half:]
    return jnp.concatenate([first * cosine - second * sine, second * cosine + first * sine], axis=-1)

def masked_weights(scores, valid):
    top = lax.optimization_barrier(jnp.max(jnp.where(valid, scores, -1e+30), axis=-1, keepdims=True))
    expd = jnp.where(valid, jnp.exp(scores - top), 0.0)
    total = lax.optimization_barrier(jnp.sum(expd, axis=-1, keepdims=True))
    return (expd / jnp.maximum(total, 1.0)).astype(jnp.bfloat16)

def compress(raw, weight_in, weight_out):
    length, groups, width = raw.shape
    block_count = length // SLC_BLOCK
    per_block = SLC_BLOCK // CMP_STRIDE
    blocked = raw.reshape(block_count, SLC_BLOCK, groups, width)
    padded = jnp.concatenate([jnp.zeros((block_count, CMP_STRIDE, groups, width), raw.dtype), blocked], axis=1)
    count = block_count * per_block
    front = padded[:, :SLC_BLOCK].reshape(count, CMP_STRIDE, groups, width)
    back = padded[:, CMP_STRIDE:].reshape(count, CMP_STRIDE, groups, width)
    window = jnp.concatenate([front, back], axis=1).transpose(0, 2, 1, 3).reshape(count * groups, CMP_BLOCK * width)
    inner = jax.nn.gelu(jnp.dot(window, weight_in, preferred_element_type=jnp.float32)).astype(jnp.bfloat16)
    return jnp.dot(inner, weight_out, preferred_element_type=jnp.float32).reshape(count, groups, width)

def reference(hidden_in, w_query, w_cmp_key, w_cmp_value, w_sel_key, w_sel_value, w_gate, cmp_key_in, cmp_key_out, cmp_value_in, cmp_value_out, out_gain, w_out, seq_lengths, chosen):
    count = SEQ_LEN // CMP_STRIDE
    per_group = HEADS // GROUPS
    scale = HEAD_DIM ** (-0.5)
    entry = jnp.arange(count).astype(jnp.int32)
    ends = entry * CMP_STRIDE + CMP_STRIDE - 1

    def one_sequence(args):
        tokens, length, picks = args
        positions = jnp.arange(SEQ_LEN).astype(jnp.int32)

        def project(weight_matrix, heads):
            return jnp.dot(tokens, weight_matrix, preferred_element_type=jnp.float32).reshape(SEQ_LEN, heads, HEAD_DIM)
        queries = rotate(project(w_query, HEADS), positions).astype(jnp.bfloat16)
        sel_keys = rotate(project(w_sel_key, GROUPS), positions).astype(jnp.bfloat16)
        sel_values = project(w_sel_value, GROUPS).astype(jnp.bfloat16)
        raw_keys = project(w_cmp_key, GROUPS).astype(jnp.bfloat16)
        raw_values = project(w_cmp_value, GROUPS).astype(jnp.bfloat16)
        cmp_keys = rotate(compress(raw_keys, cmp_key_in, cmp_key_out), ends).astype(jnp.bfloat16)
        cmp_values = compress(raw_values, cmp_value_in, cmp_value_out).astype(jnp.bfloat16)
        gate_logits = jnp.dot(tokens, w_gate.reshape(D, 2 * HEADS), preferred_element_type=jnp.float32)
        gates = jax.nn.sigmoid(gate_logits).reshape(SEQ_LEN, 2, HEADS)
        cmp_key_wide = cmp_keys.astype(jnp.float32)
        cmp_value_wide = cmp_values.astype(jnp.float32)
        sel_key_wide = sel_keys.astype(jnp.float32)
        sel_value_wide = sel_values.astype(jnp.float32)
        group_ids = jnp.arange(GROUPS).astype(jnp.int32)[:, None]

        def one_block(index):
            index = index.astype(jnp.int32)
            start = index * SLC_BLOCK
            block_q = lax.dynamic_slice_in_dim(queries, start, SLC_BLOCK, 0).astype(jnp.float32)
            block_q = block_q.reshape(SLC_BLOCK, GROUPS, per_group, HEAD_DIM)
            query_pos = start + jnp.arange(SLC_BLOCK).astype(jnp.int32)
            scores = jnp.einsum('qghd,egd->ghqe', block_q, cmp_key_wide) * scale
            valid = ((entry >= 1)[None, :] & (ends[None, :] <= query_pos[:, None]))[None, None]
            weights = masked_weights(scores, valid)
            cmp_out = jnp.einsum('ghqe,egd->qghd', weights.astype(jnp.float32), cmp_value_wide)
            lists = lax.dynamic_index_in_dim(picks, index, axis=0, keepdims=False)
            safe = jnp.maximum(lists, 0)
            token = safe[:, :, None] * SLC_BLOCK + jnp.arange(SLC_BLOCK).astype(jnp.int32)[None, None, :]
            token = token.reshape(GROUPS, TOPK * SLC_BLOCK)
            keys = sel_key_wide[token, group_ids]
            values = sel_value_wide[token, group_ids]
            live = jnp.repeat(lists >= 0, SLC_BLOCK, axis=1)
            valid_s = (live[:, None, :] & (token[:, None, :] <= query_pos[None, :, None]))[:, None]
            scores_s = jnp.einsum('qghd,gmd->ghqm', block_q, keys) * scale
            weights_s = masked_weights(scores_s, valid_s)
            sel_out = jnp.einsum('ghqm,gmd->qghd', weights_s.astype(jnp.float32), values)
            block_gates = lax.dynamic_slice_in_dim(gates, start, SLC_BLOCK, 0).reshape(SLC_BLOCK, 2, GROUPS, per_group, 1)
            mixed = block_gates[:, 0] * cmp_out + block_gates[:, 1] * sel_out
            mixed = jnp.where((query_pos < length)[:, None, None, None], mixed, 0.0)
            return mixed.reshape(SLC_BLOCK, HEADS * HEAD_DIM).astype(jnp.bfloat16)
        mixed = lax.map(one_block, jnp.arange(BLOCKS).astype(jnp.int32)).reshape(SEQ_LEN, HEADS * HEAD_DIM)
        wide = mixed.astype(jnp.float32)
        scaled = (wide * out_gain[None, :]).astype(jnp.bfloat16)
        row_scale = lax.rsqrt(lax.optimization_barrier(jnp.mean(wide * wide, axis=-1, keepdims=True)) + norm_eps)
        projected = jnp.dot(scaled, w_out, preferred_element_type=jnp.float32)
        return (projected * row_scale).astype(jnp.bfloat16)
    return lax.map(one_sequence, (hidden_in, seq_lengths, chosen))
```

```python
import functools

import jax
import jax.numpy as jnp
from jax import lax
from jax.experimental import pallas as pl
from jax.experimental.pallas import tpu as pltpu
from jax.sharding import PartitionSpec as P

HEADS = 16
HEAD_DIM = 64
CMP_STRIDE = 16
CMP_BLOCK = 32
TOPK = 16


theta_base = 500000.0
norm_eps = 1e-06


def rotate(values, positions):
    width = values.shape[-1]
    half = width // 2
    inverse = jnp.exp(
        -jnp.log(jnp.float32(theta_base)) * jnp.arange(0, width, 2).astype(jnp.float32) / width
    )
    angle = positions.astype(jnp.float32)[:, None] * inverse[None, :]
    cosine = jnp.cos(angle)[:, None, :]
    sine = jnp.sin(angle)[:, None, :]
    first = values[..., :half]
    second = values[..., half:]
    return jnp.concatenate(
        [first * cosine - second * sine, second * cosine + first * sine], axis=-1
    )


def masked_weights(scores, valid):
    top = jnp.max(jnp.where(valid, scores, -1e30), axis=-1, keepdims=True)
    expd = jnp.where(valid, jnp.exp(scores - top), 0.0)
    total = jnp.sum(expd, axis=-1, keepdims=True)
    return (expd / jnp.maximum(total, 1.0)).astype(jnp.bfloat16)


def compress(raw, prior, weight_in, weight_out):
    seqs, span, groups, width = raw.shape
    extended = jnp.concatenate([prior, raw], axis=1)
    count = span // CMP_STRIDE
    front = extended[:, :span].reshape(seqs, count, CMP_STRIDE, groups, width)
    back = extended[:, CMP_STRIDE:].reshape(seqs, count, CMP_STRIDE, groups, width)
    window = jnp.concatenate([front, back], axis=2).transpose(0, 1, 3, 2, 4)
    window = window.reshape(seqs * count * groups, CMP_BLOCK * width)
    inner = jax.nn.gelu(jnp.dot(window, weight_in, preferred_element_type=jnp.float32)).astype(
        jnp.bfloat16
    )
    return jnp.dot(inner, weight_out, preferred_element_type=jnp.float32).reshape(
        seqs, count, groups, width
    )


def shards(
    hidden_in,
    w_query,
    w_cmp_key,
    w_cmp_value,
    w_sel_key,
    w_sel_value,
    w_gate,
    cmp_key_in,
    cmp_key_out,
    cmp_value_in,
    cmp_value_out,
    out_gain,
    w_out,
    seq_lengths,
    chosen,
):
    seqs, span, width = hidden_in.shape
    block_list = lax.axis_size("kv")
    place = lax.axis_index("kv")
    column = lax.axis_index("tp")
    local_heads = w_query.shape[1] // HEAD_DIM
    local_groups = w_sel_key.shape[1] // HEAD_DIM
    per_group = local_heads // local_groups
    count = span // CMP_STRIDE
    scale = HEAD_DIM ** (-0.5)
    rows = hidden_in.reshape(seqs * span, width)
    positions = place * span + jnp.arange(span, dtype=jnp.int32)

    def project(weight_matrix, heads):
        return jnp.dot(rows, weight_matrix, preferred_element_type=jnp.float32).reshape(
            seqs, span, heads, HEAD_DIM
        )

    queries = rotate(project(w_query, local_heads), positions).astype(jnp.bfloat16)
    sel_pairs = jnp.concatenate(
        [rotate(project(w_sel_key, local_groups), positions), project(w_sel_value, local_groups)],
        axis=-1,
    ).astype(jnp.bfloat16)
    raw_pairs = jnp.concatenate(
        [project(w_cmp_key, local_groups), project(w_cmp_value, local_groups)], axis=-1
    ).astype(jnp.bfloat16)
    prior = jnp.zeros((seqs, CMP_STRIDE, local_groups, HEAD_DIM), jnp.bfloat16)
    ends = place * span + jnp.arange(count, dtype=jnp.int32) * CMP_STRIDE + CMP_STRIDE - 1
    cmp_keys = rotate(compress(raw_pairs[..., :HEAD_DIM], prior, cmp_key_in, cmp_key_out), ends)
    cmp_values = compress(raw_pairs[..., HEAD_DIM:], prior, cmp_value_in, cmp_value_out)
    cmp_piece = jnp.concatenate(
        [cmp_keys.astype(jnp.bfloat16), cmp_values.astype(jnp.bfloat16)], axis=-1
    )[:, None]
    picks = chosen[:, 0]
    every_list = lax.all_gather(picks[None, :, :, 1:], "kv", axis=0, tiled=True)
    named = jnp.any(every_list == place, axis=(0, 3)).astype(jnp.int32)
    seq_ids = jnp.arange(seqs, dtype=jnp.int32)[:, None]
    exported_seq = jnp.sum(named * seq_ids, axis=0)
    selector = seq_ids == exported_seq[None, :]
    export = jnp.sum(
        jnp.where(selector[:, None, :, None], sel_pairs, jnp.zeros((), jnp.bfloat16)), axis=0
    )
    export = export[None]
    remote_pairs, remote_entries = (
        lax.all_gather(export, "kv", axis=0, tiled=True),
        lax.all_gather(cmp_piece, "kv", axis=1, tiled=True),
    )
    gate_all = jnp.dot(rows, w_gate.reshape(width, 2 * HEADS), preferred_element_type=jnp.float32)
    gate_all = gate_all.reshape(seqs, span, 2, HEADS)
    gates = jax.nn.sigmoid(lax.dynamic_slice_in_dim(gate_all, column * local_heads, local_heads, 3))
    entry = jnp.arange(block_list * count, dtype=jnp.int32)
    entry_end = entry * CMP_STRIDE + CMP_STRIDE - 1
    cmp_valid = ((entry >= 1)[None, :] & (entry_end[None, :] <= positions[:, None]))[None, None]
    key_pos = jnp.arange(span, dtype=jnp.int32)
    own_valid = key_pos[None, :] <= key_pos[:, None]

    def one_sequence(args):
        seq_queries, seq_entries, seq_picks, seq_pairs, seq_gates, seq_length = args
        block_q = seq_queries.reshape(span, local_groups, per_group, HEAD_DIM)
        entries = seq_entries.reshape(block_list * count, local_groups, 2 * HEAD_DIM)
        scores = (
            jnp.einsum(
                "qghd,egd->ghqe",
                block_q,
                entries[..., :HEAD_DIM],
                preferred_element_type=jnp.float32,
            )
            * scale
        )
        weights = masked_weights(scores, cmp_valid)
        cmp_out = jnp.einsum(
            "ghqe,egd->qghd", weights, entries[..., HEAD_DIM:], preferred_element_type=jnp.float32
        )
        far = jnp.maximum(seq_picks[:, 1:], 0)
        fetched = jax.vmap(lambda table, index: table[index], in_axes=(2, 0))(remote_pairs, far)
        near = jnp.transpose(seq_pairs, (1, 0, 2))[:, None]
        pairs = jnp.concatenate([near, fetched], axis=1).reshape(
            local_groups, TOPK * span, 2 * HEAD_DIM
        )
        far_live = jnp.broadcast_to(
            (seq_picks[:, 1:] >= 0)[:, None, :, None], (local_groups, span, TOPK - 1, span)
        )
        near_live = jnp.broadcast_to(own_valid[None, :, None, :], (local_groups, span, 1, span))
        sel_valid = jnp.concatenate([near_live, far_live], axis=2).reshape(
            local_groups, 1, span, TOPK * span
        )
        scores_s = (
            jnp.einsum(
                "qghd,gmd->ghqm", block_q, pairs[..., :HEAD_DIM], preferred_element_type=jnp.float32
            )
            * scale
        )
        weights_s = masked_weights(scores_s, sel_valid)
        sel_out = jnp.einsum(
            "ghqm,gmd->qghd", weights_s, pairs[..., HEAD_DIM:], preferred_element_type=jnp.float32
        )
        split = seq_gates.reshape(span, 2, local_groups, per_group, 1)
        mixed = split[:, 0] * cmp_out + split[:, 1] * sel_out
        mixed = jnp.where((positions < seq_length)[:, None, None, None], mixed, 0.0)
        return mixed.reshape(span, local_heads * HEAD_DIM).astype(jnp.bfloat16)

    mixed = lax.map(one_sequence, (queries, remote_entries, picks, sel_pairs, gates, seq_lengths))
    mixed = mixed.reshape(seqs * span, local_heads * HEAD_DIM)
    out_width = width // lax.axis_size("tp")
    own_columns = lax.dynamic_slice_in_dim(w_out, column * out_width, out_width, 1)
    piece_wide = lax.all_gather(mixed, "tp", axis=1, tiled=True).astype(jnp.float32)
    scaled_piece = (piece_wide * out_gain[None, :]).astype(jnp.bfloat16)
    total = jnp.dot(scaled_piece, own_columns, preferred_element_type=jnp.float32)
    squares = jnp.sum(piece_wide * piece_wide, axis=-1)
    row_scale = lax.rsqrt(squares / (HEADS * HEAD_DIM) + norm_eps)
    return (total * row_scale[:, None]).astype(jnp.bfloat16).reshape(seqs, span, out_width)


FAR = -1e30
PLANE = 4
BLOB_EXTRA = 2
VMEM_BYTES = 60 * 1024 * 1024
f32 = jnp.float32
bf16 = jnp.bfloat16


def dot(a, b):
    return jnp.dot(a, b, preferred_element_type=f32)


def dot_t(a, b):
    return lax.dot_general(a, b, (((1,), (1,)), ((), ())), preferred_element_type=f32)


def turn(values, cosine, sine):
    lane = lax.broadcasted_iota(jnp.int32, values.shape, 1)
    other = jnp.where(
        lane % HEAD_DIM < HEAD_DIM // 2,
        pltpu.roll(values, 128 - HEAD_DIM // 2, 1),
        pltpu.roll(values, HEAD_DIM // 2, 1),
    )
    return values * cosine + other * sine


def gelu(x):
    return 0.5 * x * (1.0 + jnp.tanh(0.7978845608028654 * (x + 0.044715 * (x * x * x))))


def project_kernel(
    seqs, span, steps,
    rows_ref, wq_ref, wck_ref, wcv_ref, wsk_ref, wsv_ref, wg_ref, tables_ref, cout_ref,
    ckin_ref, cvin_ref,
    q_ref, sk_ref, sv_ref, ck_ref, cv_ref, gate_ref,
    acc_q, acc_p, acc_g, raw, kin, vin, sems,
):
    step = pl.program_id(0)
    load_k = pltpu.make_async_copy(ckin_ref, kin, sems.at[0])
    load_v = pltpu.make_async_copy(cvin_ref, vin, sems.at[1])

    @pl.when(step == 0)
    def _():
        load_k.start()
        load_v.start()
        acc_q[...] = jnp.zeros_like(acc_q)
        acc_p[...] = jnp.zeros_like(acc_p)
        acc_g[...] = jnp.zeros_like(acc_g)

    rows = rows_ref[...]
    acc_q[...] += dot(rows, wq_ref[...])
    for i, ref in enumerate((wck_ref, wcv_ref, wsk_ref, wsv_ref)):
        acc_p[i] += dot(rows, ref[...])
    acc_g[...] += dot(rows, wg_ref[...])

    @pl.when(step == steps - 1)
    def _():
        count = span // CMP_STRIDE
        entries = seqs * count
        cosine = tables_ref[0, :span]
        sine = tables_ref[1, :span]
        heads = acc_q.shape[1] // HEAD_DIM
        lane = lax.broadcasted_iota(jnp.int32, (span, 128), 1)
        low = lane < HEAD_DIM
        gate_ref[...] = jax.nn.sigmoid(acc_g[...])
        for s in range(seqs):
            part = pl.ds(s * span, span)
            sk_ref[part, :] = turn(acc_p[2, part, :], cosine, sine).astype(bf16)
            for i in range(heads // 2):
                x = turn(acc_q[part, i * 128 : (i + 1) * 128], cosine, sine)
                x = x * (HEAD_DIM**-0.5)
                y = pltpu.roll(x, HEAD_DIM, 1)
                if 2 * i < heads // 2:
                    even, odd = jnp.where(low, x, 0.0), jnp.where(low, y, 0.0)
                else:
                    even, odd = jnp.where(low, 0.0, y), jnp.where(low, 0.0, x)
                base = (s * heads + 2 * i) * span
                q_ref[base : base + span, :] = even.astype(bf16)
                q_ref[base + span : base + 2 * span, :] = odd.astype(bf16)
        sv_ref[...] = acc_p[3].astype(bf16)
        raw[...] = acc_p[0:2].astype(bf16).astype(f32)
        low_e = lax.broadcasted_iota(jnp.int32, (entries, 128), 1) < HEAD_DIM
        first = lax.broadcasted_iota(jnp.int32, (entries, 128), 0) % count == 0
        load_k.wait()
        load_v.wait()
        half = CMP_STRIDE * HEAD_DIM
        for branch, weight, out_ref in ((0, kin, ck_ref), (1, vin, cv_ref)):
            left, right = [], []
            for j in range(0, CMP_STRIDE, 2):
                a = raw[branch, pl.ds(j, entries, stride=CMP_STRIDE), :]
                b = raw[branch, pl.ds(j + 1, entries, stride=CMP_STRIDE), :]
                left.append(jnp.where(low_e, a, pltpu.roll(b, HEAD_DIM, 1)))
                right.append(jnp.where(low_e, pltpu.roll(a, HEAD_DIM, 1), b))
            window = jnp.concatenate(
                [jnp.concatenate(left, axis=1), jnp.concatenate(right, axis=1)], axis=0
            ).astype(bf16)
            front = dot(window, weight[:half])
            back = dot(window, weight[half:])
            parts = []
            for g in range(2):
                shifted = pltpu.roll(front[g * entries : (g + 1) * entries], 1, 0)
                parts.append(back[g * entries : (g + 1) * entries] + jnp.where(first, 0.0, shifted))
            inner = gelu(jnp.concatenate(parts, axis=0)).astype(bf16)
            made = dot(inner, cout_ref[branch])
            made = jnp.where(low_e, made[:entries], made[entries:])
            if branch == 0:
                made = turn(made, tables_ref[0, span:], tables_ref[1, span:])
            out_ref[...] = made.astype(bf16)


def gather_kernel(
    n, seqs, span,
    picks_ref, sk_ref, sv_ref, ck_ref, cv_ref,
    all_ref,
    lists, pick_send, pick_recv, send, recv,
):
    me = lax.axis_index("kv")
    planes = n // PLANE
    z, x, c = me // PLANE, (me // 2) % 2, me % 2
    barrier = pltpu.get_barrier_semaphore()
    for d in range(1, n):
        pl.semaphore_signal(
            barrier, inc=1, device_id={"kv": (me + d) % n},
            device_id_type=pl.DeviceIdType.MESH,
        )
    pl.semaphore_wait(barrier, n - 1)

    sent = []
    for d in range(1, n):
        copy = pltpu.make_async_remote_copy(
            src_ref=picks_ref, dst_ref=lists.at[me], send_sem=pick_send.at[d - 1],
            recv_sem=pick_recv.at[me], device_id={"kv": (me + d) % n},
            device_id_type=pl.DeviceIdType.MESH,
        )
        copy.start()
        sent.append(copy)

    entries = ck_ref.shape[0]
    all_ref[me, 2 * span : 2 * span + entries, :] = ck_ref[...]
    all_ref[me, 2 * span + entries :, :] = cv_ref[...]

    named = jnp.zeros((1, 128), jnp.int32)
    for d in range(1, n):
        origin = (me + d) % n
        pltpu.make_async_remote_copy(
            src_ref=picks_ref, dst_ref=lists.at[origin], send_sem=pick_send.at[d - 1],
            recv_sem=pick_recv.at[origin], device_id={"kv": origin},
            device_id_type=pl.DeviceIdType.MESH,
        ).wait_recv()
        named = jnp.maximum(named, (lists[origin] == me).astype(jnp.int32))
    at = lax.broadcasted_iota(jnp.int32, (1, 128), 1)
    low = at < HEAD_DIM
    named = jnp.where(at % TOPK == 0, 0, named)
    key = jnp.zeros((span, 128), f32)
    value = jnp.zeros((span, 128), f32)
    for s in range(seqs):
        flags = [
            jnp.max(jnp.where(at // TOPK == s * 2 + g, named, 0), axis=1, keepdims=True)
            for g in range(2)
        ]
        flag = jnp.where(low, flags[0], flags[1]) > 0
        key = jnp.where(flag, sk_ref[s * span : (s + 1) * span, :].astype(f32), key)
        value = jnp.where(flag, sv_ref[s * span : (s + 1) * span, :].astype(f32), value)
    all_ref[me, 0:span, :] = key.astype(bf16)
    all_ref[me, span : 2 * span, :] = value.astype(bf16)

    def pass_on(slot, dst, number):
        copy = pltpu.make_async_remote_copy(
            src_ref=all_ref.at[slot], dst_ref=all_ref.at[slot], send_sem=send.at[number],
            recv_sem=recv.at[slot], device_id={"kv": dst},
            device_id_type=pl.DeviceIdType.MESH,
        )
        copy.start()
        sent.append(copy)

    def arrived(slot):
        pltpu.make_async_remote_copy(
            src_ref=all_ref.at[slot], dst_ref=all_ref.at[slot], send_sem=send.at[0],
            recv_sem=recv.at[slot], device_id={"kv": (me + 1) % n},
            device_id_type=pl.DeviceIdType.MESH,
        ).wait_recv()

    across = z * PLANE + (1 - x) * 2 + c
    beside = z * PLANE + x * 2 + (1 - c)
    number = 0
    for d in range(1, planes):
        pass_on(me, ((z + d) % planes) * PLANE + x * 2 + c, number)
        number += 1
    pass_on(me, across, number)
    pass_on(me, beside, number + 1)
    number += 2
    order = [0] + [d for d in range(1, planes)]
    for d in order:
        origin = ((z + planes - d) % planes) * PLANE
        if d > 0:
            slot = origin + x * 2 + c
            arrived(slot)
            pass_on(slot, across, number)
            pass_on(slot, beside, number + 1)
            number += 2
    for d in order:
        origin = ((z + planes - d) % planes) * PLANE
        slot = origin + (1 - x) * 2 + c
        arrived(slot)
        pass_on(slot, beside, number)
        number += 1
    for d in order:
        origin = ((z + planes - d) % planes) * PLANE
        arrived(origin + x * 2 + (1 - c))
        arrived(origin + (1 - x) * 2 + (1 - c))
    for copy in sent:
        copy.wait_send()


def attend_kernel(
    n, seqs, span, heads,
    lens_ref, q_ref, sk_ref, sv_ref, all_ref, picks_ref, gate_ref, gain_ref, wout_ref,
    out_ref,
    weight, own, other, bias, near, wsem, send, recv,
):
    place = lax.axis_index("kv")
    column = lax.axis_index("tp")
    depth = heads * HEAD_DIM
    wide = out_ref.shape[1]
    loads = []
    for i in range(2):
        side = column if i == 0 else 1 - column
        load = pltpu.make_async_copy(
            wout_ref.at[
                pl.ds(pl.multiple_of(side * depth, depth), depth),
                pl.ds(pl.multiple_of(column * wide, wide), wide),
            ],
            weight.at[i],
            wsem.at[i],
        )
        load.start()
        loads.append(load)
    barrier = pltpu.get_barrier_semaphore()
    pl.semaphore_signal(
        barrier, inc=1, device_id={"tp": 1 - column}, device_id_type=pl.DeviceIdType.MESH
    )

    count = span // CMP_STRIDE
    entries = seqs * count
    far_keys = n * span
    block = lax.broadcasted_iota(jnp.int32, (seqs * 2, far_keys), 1) // span
    hit = jnp.zeros((seqs * 2, far_keys), jnp.int32)
    lists = picks_ref[...]
    for j in range(1, TOPK):
        hit = jnp.where(block == lists[:, j : j + 1], 1, hit)
    bias[...] = jnp.where(hit > 0, 0.0, FAR)
    row_q = lax.broadcasted_iota(jnp.int32, (span, span), 0)
    near[...] = jnp.where(
        lax.broadcasted_iota(jnp.int32, (span, span), 1) <= row_q, 0.0, FAR
    )
    slot = lax.broadcasted_iota(jnp.int32, (span, n * entries), 1)
    entry = (slot // entries) * count + slot % count
    entry_seq = (slot % entries) // count
    at = place * span + lax.broadcasted_iota(jnp.int32, (span, n * entries), 0)
    entry_ok = (entry >= 1) & (entry * CMP_STRIDE + CMP_STRIDE - 1 <= at)
    low = lax.broadcasted_iota(jnp.int32, (span, 128), 1) < HEAD_DIM
    row_at = place * span + lax.broadcasted_iota(jnp.int32, (span, 128), 0)
    far_k = all_ref[:, 0:span, :].reshape(far_keys, 128)
    far_v = all_ref[:, span : 2 * span, :].reshape(far_keys, 128)
    cmp_k = all_ref[:, 2 * span : 2 * span + entries, :].reshape(n * entries, 128)
    cmp_v = all_ref[:, 2 * span + entries :, :].reshape(n * entries, 128)
    pl.semaphore_wait(barrier, 1)

    def piece(s):
        return pltpu.make_async_remote_copy(
            src_ref=own.at[s], dst_ref=other.at[s], send_sem=send.at[s], recv_sem=recv.at[s],
            device_id={"tp": 1 - column}, device_id_type=pl.DeviceIdType.MESH,
        )

    half = heads // 2

    def one_sequence(s, carry):
        rows = pl.ds(pl.multiple_of(s * span, span), span)
        near_k = sk_ref[rows, :]
        near_v = sv_ref[rows, :]
        gates = gate_ref[rows, :]
        length = lens_ref[s]
        live = row_at < length
        entry_bias = jnp.where(entry_ok & (entry_seq == s), 0.0, FAR)
        for g in range(2):
            start = pl.multiple_of((s * heads + g * half) * span, span)
            q = q_ref[pl.ds(start, half * span), :]
            sc = dot_t(q, cmp_k).reshape(half, span, n * entries) + entry_bias[None]
            top = jnp.maximum(jnp.max(sc, axis=-1, keepdims=True), -1e29)
            e = jnp.exp(sc - top)
            total = jnp.maximum(jnp.sum(e, axis=-1, keepdims=True), 1.0)
            w = (e * (1.0 / total)).astype(bf16).reshape(half * span, n * entries)
            cmp_out = dot(w, cmp_v)
            sf = dot_t(q, far_k) + bias[pl.ds(s * 2 + g, 1), :]
            sn = (dot_t(q, near_k).reshape(half, span, span) + near[...][None]).reshape(
                half * span, span
            )
            top = jnp.maximum(
                jnp.max(sf, axis=-1, keepdims=True), jnp.max(sn, axis=-1, keepdims=True)
            )
            ef = jnp.exp(sf - top)
            en = jnp.exp(sn - top)
            total = jnp.sum(ef, axis=-1, keepdims=True) + jnp.sum(en, axis=-1, keepdims=True)
            inverse = 1.0 / total
            sel_out = dot((ef * inverse).astype(bf16), far_v) + dot(
                (en * inverse).astype(bf16), near_v
            )
            mixed = []
            for h in range(half):
                part = slice(h * span, (h + 1) * span)
                head = g * half + h
                mixed.append(
                    gates[:, head : head + 1] * cmp_out[part]
                    + gates[:, heads + head : heads + head + 1] * sel_out[part]
                )
            for h in range(0, half, 2):
                if g == 0:
                    pair = jnp.where(low, mixed[h], pltpu.roll(mixed[h + 1], HEAD_DIM, 1))
                else:
                    pair = jnp.where(low, pltpu.roll(mixed[h], HEAD_DIM, 1), mixed[h + 1])
                pair = jnp.where(live, pair, 0.0).astype(bf16)
                lanes = (g * half + h) * HEAD_DIM
                own[s, :, lanes : lanes + 128] = pair
        piece(s).start()
        return carry

    lax.fori_loop(0, seqs, one_sequence, 0)
    for load in loads:
        load.wait()
    gain_own = gain_ref[pl.ds(column, 1), :]
    gain_other = gain_ref[pl.ds(1 - column, 1), :]

    def finish(s, carry):
        piece(s).wait_recv()
        a = own[s].astype(f32)
        b = other[s].astype(f32)
        squares = jnp.sum(a * a, axis=-1, keepdims=True) + jnp.sum(b * b, axis=-1, keepdims=True)
        row_scale = lax.rsqrt(squares / (2 * depth) + norm_eps)
        total = dot((a * gain_own).astype(bf16), weight[0]) + dot(
            (b * gain_other).astype(bf16), weight[1]
        )
        out_ref[pl.ds(pl.multiple_of(s * span, span), span), :] = (total * row_scale).astype(bf16)
        return carry

    lax.fori_loop(0, seqs, finish, 0)

    def close(s, carry):
        piece(s).wait_send()
        return carry

    lax.fori_loop(0, seqs, close, 0)


def fused_shards(
    hidden_in,
    w_query,
    w_cmp_key,
    w_cmp_value,
    w_sel_key,
    w_sel_value,
    w_gate,
    cmp_key_in,
    cmp_key_out,
    cmp_value_in,
    cmp_value_out,
    out_gain,
    w_out,
    seq_lengths,
    chosen,
):
    seqs, span, width = hidden_in.shape
    n = lax.axis_size("kv")
    place = lax.axis_index("kv")
    column = lax.axis_index("tp")
    heads = w_query.shape[1] // HEAD_DIM
    count = span // CMP_STRIDE
    entries = seqs * count
    total = seqs * span
    out_width = width // lax.axis_size("tp")
    vmem = pl.BlockSpec(memory_space=pltpu.VMEM)
    anywhere = pl.BlockSpec(memory_space=pl.ANY)

    rows = hidden_in.reshape(total, width)
    gate_weight = lax.dynamic_slice_in_dim(w_gate, column * heads, heads, 2).reshape(
        width, 2 * heads
    )
    positions = place * span + jnp.concatenate(
        [
            jnp.arange(span, dtype=jnp.int32),
            jnp.tile(jnp.arange(count, dtype=jnp.int32) * CMP_STRIDE + CMP_STRIDE - 1, seqs),
        ]
    )
    lane = jnp.arange(128, dtype=jnp.int32)
    power = (lane % (HEAD_DIM // 2) * 2).astype(f32)
    inverse = jnp.exp(-jnp.log(f32(theta_base)) * power / HEAD_DIM)
    angle = positions.astype(f32)[:, None] * inverse[None, :]
    sign = jnp.where(lane % HEAD_DIM < HEAD_DIM // 2, -1.0, 1.0)
    tables = jnp.stack([jnp.cos(angle), jnp.sin(angle) * sign[None, :]])
    second = jnp.stack(
        [
            jnp.concatenate([cmp_key_out, cmp_key_out], axis=1),
            jnp.concatenate([cmp_value_out, cmp_value_out], axis=1),
        ]
    )

    steps = 4
    depth = width // steps

    def by_depth(weight_matrix):
        return pl.BlockSpec((depth, weight_matrix.shape[1]), lambda k: (k, 0))

    def whole(*shape):
        return pl.BlockSpec(shape, lambda k: (0,) * len(shape))

    small = w_sel_key.shape[1]
    q, sk, sv, ck, cv, gates = pl.pallas_call(
        functools.partial(project_kernel, seqs, span, steps),
        grid=(steps,),
        in_specs=[
            pl.BlockSpec((total, depth), lambda k: (0, k)),
            by_depth(w_query),
            by_depth(w_cmp_key),
            by_depth(w_cmp_value),
            by_depth(w_sel_key),
            by_depth(w_sel_value),
            by_depth(gate_weight),
            whole(*tables.shape),
            whole(*second.shape),
            anywhere,
            anywhere,
        ],
        out_specs=[
            whole(heads * total, 128),
            whole(total, small),
            whole(total, small),
            whole(entries, small),
            whole(entries, small),
            whole(total, 2 * heads),
        ],
        out_shape=[
            jax.ShapeDtypeStruct((heads * total, 128), bf16),
            jax.ShapeDtypeStruct((total, small), bf16),
            jax.ShapeDtypeStruct((total, small), bf16),
            jax.ShapeDtypeStruct((entries, small), bf16),
            jax.ShapeDtypeStruct((entries, small), bf16),
            jax.ShapeDtypeStruct((total, 2 * heads), f32),
        ],
        scratch_shapes=[
            pltpu.VMEM((total, heads * HEAD_DIM), f32),
            pltpu.VMEM((4, total, small), f32),
            pltpu.VMEM((total, 2 * heads), f32),
            pltpu.VMEM((2, total, small), f32),
            pltpu.VMEM(cmp_key_in.shape, bf16),
            pltpu.VMEM(cmp_value_in.shape, bf16),
            pltpu.SemaphoreType.DMA((2,)),
        ],
        compiler_params=pltpu.CompilerParams(dimension_semantics=("arbitrary",)),
        name="project",
    )(
        rows, w_query, w_cmp_key, w_cmp_value, w_sel_key, w_sel_value, gate_weight,
        tables, second, cmp_key_in, cmp_value_in,
    )

    picks = chosen[:, 0]
    blob = 2 * span + 2 * entries
    everything = pl.pallas_call(
        functools.partial(gather_kernel, n, seqs, span),
        in_specs=[vmem] * 5,
        out_specs=vmem,
        out_shape=jax.ShapeDtypeStruct((n, blob, small), bf16),
        scratch_shapes=[
            pltpu.VMEM((n, 1, 128), jnp.int32),
            pltpu.SemaphoreType.DMA((n,)),
            pltpu.SemaphoreType.DMA((n,)),
            pltpu.SemaphoreType.DMA((n,)),
            pltpu.SemaphoreType.DMA((n,)),
        ],
        compiler_params=pltpu.CompilerParams(collective_id=0, has_side_effects=True),
        name="gather",
    )(picks.reshape(1, 128), sk, sv, ck, cv)

    out = pl.pallas_call(
        functools.partial(attend_kernel, n, seqs, span, heads),
        in_specs=[pl.BlockSpec(memory_space=pltpu.SMEM)] + [vmem] * 7 + [anywhere],
        out_specs=vmem,
        out_shape=jax.ShapeDtypeStruct((total, out_width), bf16),
        scratch_shapes=[
            pltpu.VMEM((2, heads * HEAD_DIM, out_width), bf16),
            pltpu.VMEM((seqs, span, heads * HEAD_DIM), bf16),
            pltpu.VMEM((seqs, span, heads * HEAD_DIM), bf16),
            pltpu.VMEM((seqs * 2, n * span), f32),
            pltpu.VMEM((span, span), f32),
            pltpu.SemaphoreType.DMA((2,)),
            pltpu.SemaphoreType.DMA((seqs,)),
            pltpu.SemaphoreType.DMA((seqs,)),
        ],
        compiler_params=pltpu.CompilerParams(
            collective_id=1, has_side_effects=True, vmem_limit_bytes=VMEM_BYTES
        ),
        name="attend",
    )(
        seq_lengths, q, sk, sv, everything, picks.reshape(seqs * 2, TOPK), gates,
        out_gain.reshape(2, heads * HEAD_DIM), w_out,
    )
    return out.reshape(seqs, span, out_width)


def fits(mesh):
    n = mesh.shape["kv"]
    return mesh.shape["tp"] == 2 and n % PLANE == 0 and n <= 32


def solution(mesh):
    placed = (
        P(None, "kv", None),
        P(None, "tp"),
        P(None, "tp"),
        P(None, "tp"),
        P(None, "tp"),
        P(None, "tp"),
        P(),
        P(),
        P(),
        P(),
        P(),
        P(),
        P(),
        P(),
        P(None, "kv", "tp", None),
    )
    return jax.shard_map(
        fused_shards if fits(mesh) else shards, mesh=mesh, in_specs=placed, out_specs=P(None, "kv", "tp"), check_vma=False
    )
```

```python
import functools

import jax
import jax.numpy as jnp
from jax import lax
from jax.experimental import pallas as pl
from jax.experimental.pallas import tpu as pltpu
from jax.sharding import PartitionSpec as P

HEADS = 16
HEAD_DIM = 64
CMP_STRIDE = 16
CMP_BLOCK = 32
TOPK = 16


theta_base = 500000.0
norm_eps = 1e-06


def rotate(values, positions):
    width = values.shape[-1]
    half = width // 2
    inverse = jnp.exp(
        -jnp.log(jnp.float32(theta_base)) * jnp.arange(0, width, 2).astype(jnp.float32) / width
    )
    angle = positions.astype(jnp.float32)[:, None] * inverse[None, :]
    cosine = jnp.cos(angle)[:, None, :]
    sine = jnp.sin(angle)[:, None, :]
    first = values[..., :half]
    second = values[..., half:]
    return jnp.concatenate(
        [first * cosine - second * sine, second * cosine + first * sine], axis=-1
    )


def masked_weights(scores, valid):
    top = jnp.max(jnp.where(valid, scores, -1e30), axis=-1, keepdims=True)
    expd = jnp.where(valid, jnp.exp(scores - top), 0.0)
    total = jnp.sum(expd, axis=-1, keepdims=True)
    return (expd / jnp.maximum(total, 1.0)).astype(jnp.bfloat16)


def compress(raw, prior, weight_in, weight_out):
    seqs, span, groups, width = raw.shape
    extended = jnp.concatenate([prior, raw], axis=1)
    count = span // CMP_STRIDE
    front = extended[:, :span].reshape(seqs, count, CMP_STRIDE, groups, width)
    back = extended[:, CMP_STRIDE:].reshape(seqs, count, CMP_STRIDE, groups, width)
    window = jnp.concatenate([front, back], axis=2).transpose(0, 1, 3, 2, 4)
    window = window.reshape(seqs * count * groups, CMP_BLOCK * width)
    inner = jax.nn.gelu(jnp.dot(window, weight_in, preferred_element_type=jnp.float32)).astype(
        jnp.bfloat16
    )
    return jnp.dot(inner, weight_out, preferred_element_type=jnp.float32).reshape(
        seqs, count, groups, width
    )


def shards(
    hidden_in,
    w_query,
    w_cmp_key,
    w_cmp_value,
    w_sel_key,
    w_sel_value,
    w_gate,
    cmp_key_in,
    cmp_key_out,
    cmp_value_in,
    cmp_value_out,
    out_gain,
    w_out,
    seq_lengths,
    chosen,
):
    seqs, span, width = hidden_in.shape
    block_list = lax.axis_size("kv")
    place = lax.axis_index("kv")
    column = lax.axis_index("tp")
    local_heads = w_query.shape[1] // HEAD_DIM
    local_groups = w_sel_key.shape[1] // HEAD_DIM
    per_group = local_heads // local_groups
    count = span // CMP_STRIDE
    scale = HEAD_DIM ** (-0.5)
    rows = hidden_in.reshape(seqs * span, width)
    positions = place * span + jnp.arange(span, dtype=jnp.int32)

    def project(weight_matrix, heads):
        return jnp.dot(rows, weight_matrix, preferred_element_type=jnp.float32).reshape(
            seqs, span, heads, HEAD_DIM
        )

    queries = rotate(project(w_query, local_heads), positions).astype(jnp.bfloat16)
    sel_pairs = jnp.concatenate(
        [rotate(project(w_sel_key, local_groups), positions), project(w_sel_value, local_groups)],
        axis=-1,
    ).astype(jnp.bfloat16)
    raw_pairs = jnp.concatenate(
        [project(w_cmp_key, local_groups), project(w_cmp_value, local_groups)], axis=-1
    ).astype(jnp.bfloat16)
    prior = jnp.zeros((seqs, CMP_STRIDE, local_groups, HEAD_DIM), jnp.bfloat16)
    ends = place * span + jnp.arange(count, dtype=jnp.int32) * CMP_STRIDE + CMP_STRIDE - 1
    cmp_keys = rotate(compress(raw_pairs[..., :HEAD_DIM], prior, cmp_key_in, cmp_key_out), ends)
    cmp_values = compress(raw_pairs[..., HEAD_DIM:], prior, cmp_value_in, cmp_value_out)
    cmp_piece = jnp.concatenate(
        [cmp_keys.astype(jnp.bfloat16), cmp_values.astype(jnp.bfloat16)], axis=-1
    )[:, None]
    picks = chosen[:, 0]
    every_list = lax.all_gather(picks[None, :, :, 1:], "kv", axis=0, tiled=True)
    named = jnp.any(every_list == place, axis=(0, 3)).astype(jnp.int32)
    seq_ids = jnp.arange(seqs, dtype=jnp.int32)[:, None]
    exported_seq = jnp.sum(named * seq_ids, axis=0)
    selector = seq_ids == exported_seq[None, :]
    export = jnp.sum(
        jnp.where(selector[:, None, :, None], sel_pairs, jnp.zeros((), jnp.bfloat16)), axis=0
    )
    export = export[None]
    remote_pairs, remote_entries = (
        lax.all_gather(export, "kv", axis=0, tiled=True),
        lax.all_gather(cmp_piece, "kv", axis=1, tiled=True),
    )
    gate_all = jnp.dot(rows, w_gate.reshape(width, 2 * HEADS), preferred_element_type=jnp.float32)
    gate_all = gate_all.reshape(seqs, span, 2, HEADS)
    gates = jax.nn.sigmoid(lax.dynamic_slice_in_dim(gate_all, column * local_heads, local_heads, 3))
    entry = jnp.arange(block_list * count, dtype=jnp.int32)
    entry_end = entry * CMP_STRIDE + CMP_STRIDE - 1
    cmp_valid = ((entry >= 1)[None, :] & (entry_end[None, :] <= positions[:, None]))[None, None]
    key_pos = jnp.arange(span, dtype=jnp.int32)
    own_valid = key_pos[None, :] <= key_pos[:, None]

    def one_sequence(args):
        seq_queries, seq_entries, seq_picks, seq_pairs, seq_gates, seq_length = args
        block_q = seq_queries.reshape(span, local_groups, per_group, HEAD_DIM)
        entries = seq_entries.reshape(block_list * count, local_groups, 2 * HEAD_DIM)
        scores = (
            jnp.einsum(
                "qghd,egd->ghqe",
                block_q,
                entries[..., :HEAD_DIM],
                preferred_element_type=jnp.float32,
            )
            * scale
        )
        weights = masked_weights(scores, cmp_valid)
        cmp_out = jnp.einsum(
            "ghqe,egd->qghd", weights, entries[..., HEAD_DIM:], preferred_element_type=jnp.float32
        )
        far = jnp.maximum(seq_picks[:, 1:], 0)
        fetched = jax.vmap(lambda table, index: table[index], in_axes=(2, 0))(remote_pairs, far)
        near = jnp.transpose(seq_pairs, (1, 0, 2))[:, None]
        pairs = jnp.concatenate([near, fetched], axis=1).reshape(
            local_groups, TOPK * span, 2 * HEAD_DIM
        )
        far_live = jnp.broadcast_to(
            (seq_picks[:, 1:] >= 0)[:, None, :, None], (local_groups, span, TOPK - 1, span)
        )
        near_live = jnp.broadcast_to(own_valid[None, :, None, :], (local_groups, span, 1, span))
        sel_valid = jnp.concatenate([near_live, far_live], axis=2).reshape(
            local_groups, 1, span, TOPK * span
        )
        scores_s = (
            jnp.einsum(
                "qghd,gmd->ghqm", block_q, pairs[..., :HEAD_DIM], preferred_element_type=jnp.float32
            )
            * scale
        )
        weights_s = masked_weights(scores_s, sel_valid)
        sel_out = jnp.einsum(
            "ghqm,gmd->qghd", weights_s, pairs[..., HEAD_DIM:], preferred_element_type=jnp.float32
        )
        split = seq_gates.reshape(span, 2, local_groups, per_group, 1)
        mixed = split[:, 0] * cmp_out + split[:, 1] * sel_out
        mixed = jnp.where((positions < seq_length)[:, None, None, None], mixed, 0.0)
        return mixed.reshape(span, local_heads * HEAD_DIM).astype(jnp.bfloat16)

    mixed = lax.map(one_sequence, (queries, remote_entries, picks, sel_pairs, gates, seq_lengths))
    mixed = mixed.reshape(seqs * span, local_heads * HEAD_DIM)
    out_width = width // lax.axis_size("tp")
    own_columns = lax.dynamic_slice_in_dim(w_out, column * out_width, out_width, 1)
    piece_wide = lax.all_gather(mixed, "tp", axis=1, tiled=True).astype(jnp.float32)
    scaled_piece = (piece_wide * out_gain[None, :]).astype(jnp.bfloat16)
    total = jnp.dot(scaled_piece, own_columns, preferred_element_type=jnp.float32)
    squares = jnp.sum(piece_wide * piece_wide, axis=-1)
    row_scale = lax.rsqrt(squares / (HEADS * HEAD_DIM) + norm_eps)
    return (total * row_scale[:, None]).astype(jnp.bfloat16).reshape(seqs, span, out_width)


FAR = -1e30
PLANE = 4
VMEM_BYTES = 60 * 1024 * 1024
f32 = jnp.float32
bf16 = jnp.bfloat16


def dot(a, b):
    return jnp.dot(a, b, preferred_element_type=f32)


def dot_t(a, b):
    return lax.dot_general(a, b, (((1,), (1,)), ((), ())), preferred_element_type=f32)


def turn(values, cosine, sine):
    lane = lax.broadcasted_iota(jnp.int32, values.shape, 1)
    other = jnp.where(
        lane % HEAD_DIM < HEAD_DIM // 2,
        pltpu.roll(values, 128 - HEAD_DIM // 2, 1),
        pltpu.roll(values, HEAD_DIM // 2, 1),
    )
    return values * cosine + other * sine


def gelu(x):
    return 0.5 * x * (1.0 + jnp.tanh(0.7978845608028654 * (x + 0.044715 * (x * x * x))))


def layer_kernel(
    n, seqs, span, heads,
    lens_ref, picks_ref, freq_ref, gain_ref, kout_ref, vout_ref,
    rows_ref, wq_ref, wck_ref, wcv_ref, wsk_ref, wsv_ref, wg_ref, kin_ref, vin_ref, wout_ref,
    out_ref,
    rows, wq, ws, wg, kin, vin, weight,
    q_buf, sk_buf, sv_buf, raw, gate_buf, lists, blobs, own, other, bias, near,
    load_sem, pick_send, pick_recv, blob_send, blob_recv, half_send, half_recv,
):
    me = lax.axis_index("kv")
    column = lax.axis_index("tp")
    planes = n // PLANE
    z, x, c = me // PLANE, (me // 2) % 2, me % 2
    depth = heads * HEAD_DIM
    wide = out_ref.shape[1]
    count = span // CMP_STRIDE
    entries = seqs * count
    half = heads // 2
    mesh_id = pl.DeviceIdType.MESH

    pairs = [(rows_ref, rows)]
    for i, ref in enumerate((wsk_ref, wsv_ref, wck_ref, wcv_ref)):
        pairs.append((ref, ws.at[:, i * 128 : (i + 1) * 128]))
    pairs += [(kin_ref, kin), (vin_ref, vin), (wq_ref, wq), (wg_ref, wg)]
    for i in range(2):
        side = column if i == 0 else 1 - column
        block = wout_ref.at[
            pl.ds(pl.multiple_of(side * depth, depth), depth),
            pl.ds(pl.multiple_of(column * wide, wide), wide),
        ]
        pairs.append((block, weight.at[i]))
    loads = [pltpu.make_async_copy(a, b, load_sem.at[i]) for i, (a, b) in enumerate(pairs)]
    for load in loads:
        load.start()

    barrier = pltpu.get_barrier_semaphore()
    for d in range(1, n):
        pl.semaphore_signal(
            barrier, inc=1, device_id={"kv": (me + d) % n}, device_id_type=mesh_id
        )
    pl.semaphore_signal(barrier, inc=1, device_id={"tp": 1 - column}, device_id_type=mesh_id)

    lane = lax.broadcasted_iota(jnp.int32, (span, 128), 1)
    low = lane < HEAD_DIM
    low_e = low[:entries]
    at = lax.broadcasted_iota(jnp.int32, (span, 128), 0)
    sign = jnp.where(lane % HEAD_DIM < HEAD_DIM // 2, -1.0, 1.0)
    angle = (me * span + at).astype(f32) * freq_ref[...]
    cosine = jnp.cos(angle)
    sine = jnp.sin(angle) * sign
    end = me * span + (at[:entries] % count) * CMP_STRIDE + CMP_STRIDE - 1
    angle = end.astype(f32) * freq_ref[...]
    cosine_e = jnp.cos(angle)
    sine_e = jnp.sin(angle) * sign[:entries]
    row_q = lax.broadcasted_iota(jnp.int32, (span, span), 0)
    near[...] = jnp.where(
        lax.broadcasted_iota(jnp.int32, (span, span), 1) <= row_q, 0.0, FAR
    )
    far_keys = n * span
    block = lax.broadcasted_iota(jnp.int32, (2, far_keys), 1) // span
    for s in range(seqs):
        listed = picks_ref[s]
        hit = jnp.zeros((2, far_keys), jnp.int32)
        for j in range(1, TOPK):
            hit = jnp.where(block == listed[:, j : j + 1], 1, hit)
        bias[s] = jnp.where(hit > 0, 0.0, FAR)

    pl.semaphore_wait(barrier, n)
    sent = []
    for d in range(1, n):
        copy = pltpu.make_async_remote_copy(
            src_ref=picks_ref, dst_ref=lists.at[me], send_sem=pick_send.at[d - 1],
            recv_sem=pick_recv.at[me], device_id={"kv": (me + d) % n}, device_id_type=mesh_id,
        )
        copy.start()
        sent.append(copy)

    for load in loads[:5]:
        load.wait()
    made = dot(rows[...], ws[...])
    for s in range(seqs):
        part = slice(s * span, (s + 1) * span)
        sk_buf[part, :] = turn(made[part, :128], cosine, sine).astype(bf16)
    sv_buf[...] = made[:, 128:256].astype(bf16)
    raw[0] = made[:, 256:384].astype(bf16).astype(f32)
    raw[1] = made[:, 384:512].astype(bf16).astype(f32)
    first = at[:entries] % count == 0
    mid = CMP_STRIDE * HEAD_DIM
    for branch, inner_weight, outer in ((0, kin, kout_ref), (1, vin, vout_ref)):
        loads[5 + branch].wait()
        left, right = [], []
        for j in range(0, CMP_STRIDE, 2):
            a = raw[branch, pl.ds(j, entries, stride=CMP_STRIDE), :]
            b = raw[branch, pl.ds(j + 1, entries, stride=CMP_STRIDE), :]
            left.append(jnp.where(low_e, a, pltpu.roll(b, HEAD_DIM, 1)))
            right.append(jnp.where(low_e, pltpu.roll(a, HEAD_DIM, 1), b))
        window = jnp.concatenate(
            [jnp.concatenate(left, axis=1), jnp.concatenate(right, axis=1)], axis=0
        ).astype(bf16)
        front = dot(window, inner_weight[:mid])
        back = dot(window, inner_weight[mid:])
        parts = []
        for g in range(2):
            shifted = pltpu.roll(front[g * entries : (g + 1) * entries], 1, 0)
            parts.append(back[g * entries : (g + 1) * entries] + jnp.where(first, 0.0, shifted))
        inner = gelu(jnp.concatenate(parts, axis=0)).astype(bf16)
        outer = jnp.concatenate([outer[...], outer[...]], axis=0)
        result = dot_t(inner, outer)
        result = jnp.where(low_e, result[:entries], result[entries:])
        if branch == 0:
            result = turn(result, cosine_e, sine_e)
        start = 2 * span + branch * entries
        blobs[me, start : start + entries, :] = result.astype(bf16)

    named = jnp.zeros((seqs, 2, TOPK), jnp.int32)
    for d in range(1, n):
        origin = (me + d) % n
        pltpu.make_async_remote_copy(
            src_ref=picks_ref, dst_ref=lists.at[origin], send_sem=pick_send.at[d - 1],
            recv_sem=pick_recv.at[origin], device_id={"kv": origin}, device_id_type=mesh_id,
        ).wait_recv()
        named = jnp.maximum(named, (lists[origin] == me).astype(jnp.int32))
    slot_at = lax.broadcasted_iota(jnp.int32, (seqs, 2, TOPK), 2)
    named = jnp.max(jnp.where(slot_at == 0, 0, named), axis=2, keepdims=True)
    key = jnp.zeros((span, 128), f32)
    value = jnp.zeros((span, 128), f32)
    for s in range(seqs):
        flag = jnp.where(low, named[s, 0:1, :], named[s, 1:2, :]) > 0
        key = jnp.where(flag, sk_buf[s * span : (s + 1) * span, :].astype(f32), key)
        value = jnp.where(flag, sv_buf[s * span : (s + 1) * span, :].astype(f32), value)
    blobs[me, 0:span, :] = key.astype(bf16)
    blobs[me, span : 2 * span, :] = value.astype(bf16)

    def pass_on(slot, dst, number):
        copy = pltpu.make_async_remote_copy(
            src_ref=blobs.at[slot], dst_ref=blobs.at[slot], send_sem=blob_send.at[number],
            recv_sem=blob_recv.at[slot], device_id={"kv": dst}, device_id_type=mesh_id,
        )
        copy.start()
        sent.append(copy)

    def arrived(slot):
        pltpu.make_async_remote_copy(
            src_ref=blobs.at[slot], dst_ref=blobs.at[slot], send_sem=blob_send.at[0],
            recv_sem=blob_recv.at[slot], device_id={"kv": (me + 1) % n}, device_id_type=mesh_id,
        ).wait_recv()

    across = z * PLANE + (1 - x) * 2 + c
    beside = z * PLANE + x * 2 + (1 - c)
    order = sorted(range(1, planes), key=lambda d: (min(d, planes - d), d))
    number = 0
    for d in order:
        pass_on(me, ((z + d) % planes) * PLANE + x * 2 + c, number)
        number += 1
    pass_on(me, across, number)
    pass_on(me, beside, number + 1)
    number += 2

    loads[7].wait()
    loads[8].wait()
    hidden = rows[...]
    for i in range(half):
        made = dot(hidden, wq[:, i * 128 : (i + 1) * 128])
        for s in range(seqs):
            v = turn(made[s * span : (s + 1) * span], cosine, sine) * (HEAD_DIM**-0.5)
            y = pltpu.roll(v, HEAD_DIM, 1)
            if 2 * i < half:
                even, odd = jnp.where(low, v, 0.0), jnp.where(low, y, 0.0)
            else:
                even, odd = jnp.where(low, 0.0, y), jnp.where(low, 0.0, v)
            base = (s * heads + 2 * i) * span
            q_buf[base : base + span, :] = even.astype(bf16)
            q_buf[base + span : base + 2 * span, :] = odd.astype(bf16)
    spread = 2 * wg_ref.shape[1]
    gate_buf[...] = jnp.zeros_like(gate_buf)
    gate_buf[:, :spread] = jax.nn.sigmoid(dot_t(hidden, wg[...].reshape(spread, rows.shape[1])))

    for d in order:
        slot = ((z + planes - d) % planes) * PLANE + x * 2 + c
        arrived(slot)
        pass_on(slot, across, number)
        pass_on(slot, beside, number + 1)
        number += 2
    for d in [0] + order:
        slot = ((z + planes - d) % planes) * PLANE + (1 - x) * 2 + c
        arrived(slot)
        pass_on(slot, beside, number)
        number += 1
    for d in [0] + order:
        origin = ((z + planes - d) % planes) * PLANE
        arrived(origin + x * 2 + (1 - c))
        arrived(origin + (1 - x) * 2 + (1 - c))

    slot = lax.broadcasted_iota(jnp.int32, (span, n * entries), 1)
    entry = (slot // entries) * count + slot % count
    entry_seq = (slot % entries) // count
    query_at = me * span + lax.broadcasted_iota(jnp.int32, (span, n * entries), 0)
    entry_ok = (entry >= 1) & (entry * CMP_STRIDE + CMP_STRIDE - 1 <= query_at)
    row_at = me * span + at
    far_k = blobs[:, 0:span, :].reshape(far_keys, 128)
    far_v = blobs[:, span : 2 * span, :].reshape(far_keys, 128)
    cmp_k = blobs[:, 2 * span : 2 * span + entries, :].reshape(n * entries, 128)
    cmp_v = blobs[:, 2 * span + entries :, :].reshape(n * entries, 128)

    def piece(s):
        return pltpu.make_async_remote_copy(
            src_ref=own.at[s], dst_ref=other.at[s], send_sem=half_send.at[s],
            recv_sem=half_recv.at[s], device_id={"tp": 1 - column}, device_id_type=mesh_id,
        )

    def one_sequence(s, carry):
        part = pl.ds(pl.multiple_of(s * span, span), span)
        near_k = sk_buf[part, :]
        near_v = sv_buf[part, :]
        gates = gate_buf[part, :]
        gates = jnp.where(column == 0, gates, pltpu.roll(gates, 128 - heads, 1))
        live = row_at < lens_ref[s]
        entry_bias = jnp.where(entry_ok & (entry_seq == s), 0.0, FAR)
        for g in range(2):
            start = pl.multiple_of((s * heads + g * half) * span, span)
            q = q_buf[pl.ds(start, half * span), :]
            sc = dot_t(q, cmp_k).reshape(half, span, n * entries) + entry_bias[None]
            top = jnp.maximum(jnp.max(sc, axis=-1, keepdims=True), -1e29)
            e = jnp.exp(sc - top)
            total = jnp.maximum(jnp.sum(e, axis=-1, keepdims=True), 1.0)
            w = (e * (1.0 / total)).astype(bf16).reshape(half * span, n * entries)
            cmp_out = dot(w, cmp_v)
            sf = dot_t(q, far_k) + bias[s, g : g + 1, :]
            sn = (dot_t(q, near_k).reshape(half, span, span) + near[...][None]).reshape(
                half * span, span
            )
            top = jnp.maximum(
                jnp.max(sf, axis=-1, keepdims=True), jnp.max(sn, axis=-1, keepdims=True)
            )
            ef = jnp.exp(sf - top)
            en = jnp.exp(sn - top)
            total = jnp.sum(ef, axis=-1, keepdims=True) + jnp.sum(en, axis=-1, keepdims=True)
            inverse = 1.0 / total
            sel_out = dot((ef * inverse).astype(bf16), far_v) + dot(
                (en * inverse).astype(bf16), near_v
            )
            mixed = []
            for h in range(half):
                span_h = slice(h * span, (h + 1) * span)
                head = g * half + h
                behind = spread // 2 + head
                mixed.append(
                    gates[:, head : head + 1] * cmp_out[span_h]
                    + gates[:, behind : behind + 1] * sel_out[span_h]
                )
            for h in range(0, half, 2):
                if g == 0:
                    pair = jnp.where(low, mixed[h], pltpu.roll(mixed[h + 1], HEAD_DIM, 1))
                else:
                    pair = jnp.where(low, pltpu.roll(mixed[h], HEAD_DIM, 1), mixed[h + 1])
                pair = jnp.where(live, pair, 0.0).astype(bf16)
                lanes = (g * half + h) * HEAD_DIM
                own[s, :, lanes : lanes + 128] = pair
        piece(s).start()
        return carry

    lax.fori_loop(0, seqs, one_sequence, 0)
    for load in loads[9:]:
        load.wait()
    gain_own = gain_ref[:, pl.ds(pl.multiple_of(column * depth, depth), depth)]
    gain_other = gain_ref[:, pl.ds(pl.multiple_of((1 - column) * depth, depth), depth)]

    def finish(s, carry):
        piece(s).wait_recv()
        a = own[s].astype(f32)
        b = other[s].astype(f32)
        squares = jnp.sum(a * a, axis=-1, keepdims=True) + jnp.sum(b * b, axis=-1, keepdims=True)
        row_scale = lax.rsqrt(squares / (2 * depth) + norm_eps)
        total = dot((a * gain_own).astype(bf16), weight[0]) + dot(
            (b * gain_other).astype(bf16), weight[1]
        )
        out_ref[pl.ds(pl.multiple_of(s * span, span), span), :] = (total * row_scale).astype(bf16)
        return carry

    lax.fori_loop(0, seqs, finish, 0)

    def close(s, carry):
        piece(s).wait_send()
        return carry

    lax.fori_loop(0, seqs, close, 0)
    for copy in sent:
        copy.wait_send()


def fused_shards(
    hidden_in,
    w_query,
    w_cmp_key,
    w_cmp_value,
    w_sel_key,
    w_sel_value,
    w_gate,
    cmp_key_in,
    cmp_key_out,
    cmp_value_in,
    cmp_value_out,
    out_gain,
    w_out,
    seq_lengths,
    chosen,
):
    seqs, span, width = hidden_in.shape
    n = lax.axis_size("kv")
    heads = w_query.shape[1] // HEAD_DIM
    total = seqs * span
    entries = total // CMP_STRIDE
    out_width = width // lax.axis_size("tp")
    small = w_sel_key.shape[1]
    vmem = pl.BlockSpec(memory_space=pltpu.VMEM)
    anywhere = pl.BlockSpec(memory_space=pl.ANY)
    power = jnp.arange(128, dtype=jnp.int32) % (HEAD_DIM // 2) * 2
    freq = jnp.exp(-jnp.log(f32(theta_base)) * power.astype(f32) / HEAD_DIM)
    gate_rows = jnp.transpose(w_gate, (1, 2, 0))
    out = pl.pallas_call(
        functools.partial(layer_kernel, n, seqs, span, heads),
        in_specs=[pl.BlockSpec(memory_space=pltpu.SMEM)] + [vmem] * 5 + [anywhere] * 10,
        out_specs=vmem,
        out_shape=jax.ShapeDtypeStruct((total, out_width), bf16),
        scratch_shapes=[
            pltpu.VMEM((total, width), bf16),
            pltpu.VMEM(w_query.shape, bf16),
            pltpu.VMEM((width, 4 * small), bf16),
            pltpu.VMEM(gate_rows.shape, bf16),
            pltpu.VMEM(cmp_key_in.shape, bf16),
            pltpu.VMEM(cmp_value_in.shape, bf16),
            pltpu.VMEM((2, heads * HEAD_DIM, out_width), bf16),
            pltpu.VMEM((heads * total, 128), bf16),
            pltpu.VMEM((total, small), bf16),
            pltpu.VMEM((total, small), bf16),
            pltpu.VMEM((2, total, small), f32),
            pltpu.VMEM((total, 128), f32),
            pltpu.VMEM((n, seqs, 2, TOPK), jnp.int32),
            pltpu.VMEM((n, 2 * span + 2 * entries, small), bf16),
            pltpu.VMEM((seqs, span, heads * HEAD_DIM), bf16),
            pltpu.VMEM((seqs, span, heads * HEAD_DIM), bf16),
            pltpu.VMEM((seqs, 2, n * span), f32),
            pltpu.VMEM((span, span), f32),
            pltpu.SemaphoreType.DMA((11,)),
            pltpu.SemaphoreType.DMA((n,)),
            pltpu.SemaphoreType.DMA((n,)),
            pltpu.SemaphoreType.DMA((n,)),
            pltpu.SemaphoreType.DMA((n,)),
            pltpu.SemaphoreType.DMA((seqs,)),
            pltpu.SemaphoreType.DMA((seqs,)),
        ],
        compiler_params=pltpu.CompilerParams(
            collective_id=0, has_side_effects=True, vmem_limit_bytes=VMEM_BYTES
        ),
        name="layer",
    )(
        seq_lengths, chosen[:, 0], freq[None], out_gain[None],
        jnp.transpose(cmp_key_out), jnp.transpose(cmp_value_out),
        hidden_in.reshape(total, width), w_query, w_cmp_key, w_cmp_value, w_sel_key,
        w_sel_value, gate_rows, cmp_key_in, cmp_value_in, w_out,
    )
    return out.reshape(seqs, span, out_width)


def fits(mesh):
    n = mesh.shape["kv"]
    return mesh.shape["tp"] == 2 and n % PLANE == 0 and n <= 32


def solution(mesh):
    placed = (
        P(None, "kv", None),
        P(None, "tp"),
        P(None, "tp"),
        P(None, "tp"),
        P(None, "tp"),
        P(None, "tp"),
        P(),
        P(),
        P(),
        P(),
        P(),
        P(),
        P(),
        P(),
        P(None, "kv", "tp", None),
    )
    return jax.shard_map(
        fused_shards if fits(mesh) else shards, mesh=mesh, in_specs=placed, out_specs=P(None, "kv", "tp"), check_vma=False
    )
```

```python
import functools
import math

import jax
import jax.numpy as jnp
from jax import lax
from jax.experimental import pallas as pl
from jax.experimental.pallas import tpu as pltpu
from jax.sharding import PartitionSpec as P

HEADS = 16
HEAD_DIM = 64
CMP_STRIDE = 16
CMP_BLOCK = 32
TOPK = 16


theta_base = 500000.0
norm_eps = 1e-06


def rotate(values, positions):
    width = values.shape[-1]
    half = width // 2
    inverse = jnp.exp(
        -jnp.log(jnp.float32(theta_base)) * jnp.arange(0, width, 2).astype(jnp.float32) / width
    )
    angle = positions.astype(jnp.float32)[:, None] * inverse[None, :]
    cosine = jnp.cos(angle)[:, None, :]
    sine = jnp.sin(angle)[:, None, :]
    first = values[..., :half]
    second = values[..., half:]
    return jnp.concatenate(
        [first * cosine - second * sine, second * cosine + first * sine], axis=-1
    )


def masked_weights(scores, valid):
    top = jnp.max(jnp.where(valid, scores, -1e30), axis=-1, keepdims=True)
    expd = jnp.where(valid, jnp.exp(scores - top), 0.0)
    total = jnp.sum(expd, axis=-1, keepdims=True)
    return (expd / jnp.maximum(total, 1.0)).astype(jnp.bfloat16)


def compress(raw, prior, weight_in, weight_out):
    seqs, span, groups, width = raw.shape
    extended = jnp.concatenate([prior, raw], axis=1)
    count = span // CMP_STRIDE
    front = extended[:, :span].reshape(seqs, count, CMP_STRIDE, groups, width)
    back = extended[:, CMP_STRIDE:].reshape(seqs, count, CMP_STRIDE, groups, width)
    window = jnp.concatenate([front, back], axis=2).transpose(0, 1, 3, 2, 4)
    window = window.reshape(seqs * count * groups, CMP_BLOCK * width)
    inner = jax.nn.gelu(jnp.dot(window, weight_in, preferred_element_type=jnp.float32)).astype(
        jnp.bfloat16
    )
    return jnp.dot(inner, weight_out, preferred_element_type=jnp.float32).reshape(
        seqs, count, groups, width
    )


def shards(
    hidden_in,
    w_query,
    w_cmp_key,
    w_cmp_value,
    w_sel_key,
    w_sel_value,
    w_gate,
    cmp_key_in,
    cmp_key_out,
    cmp_value_in,
    cmp_value_out,
    out_gain,
    w_out,
    seq_lengths,
    chosen,
):
    seqs, span, width = hidden_in.shape
    block_list = lax.axis_size("kv")
    place = lax.axis_index("kv")
    column = lax.axis_index("tp")
    local_heads = w_query.shape[1] // HEAD_DIM
    local_groups = w_sel_key.shape[1] // HEAD_DIM
    per_group = local_heads // local_groups
    count = span // CMP_STRIDE
    scale = HEAD_DIM ** (-0.5)
    rows = hidden_in.reshape(seqs * span, width)
    positions = place * span + jnp.arange(span, dtype=jnp.int32)

    def project(weight_matrix, heads):
        return jnp.dot(rows, weight_matrix, preferred_element_type=jnp.float32).reshape(
            seqs, span, heads, HEAD_DIM
        )

    queries = rotate(project(w_query, local_heads), positions).astype(jnp.bfloat16)
    sel_pairs = jnp.concatenate(
        [rotate(project(w_sel_key, local_groups), positions), project(w_sel_value, local_groups)],
        axis=-1,
    ).astype(jnp.bfloat16)
    raw_pairs = jnp.concatenate(
        [project(w_cmp_key, local_groups), project(w_cmp_value, local_groups)], axis=-1
    ).astype(jnp.bfloat16)
    prior = jnp.zeros((seqs, CMP_STRIDE, local_groups, HEAD_DIM), jnp.bfloat16)
    ends = place * span + jnp.arange(count, dtype=jnp.int32) * CMP_STRIDE + CMP_STRIDE - 1
    cmp_keys = rotate(compress(raw_pairs[..., :HEAD_DIM], prior, cmp_key_in, cmp_key_out), ends)
    cmp_values = compress(raw_pairs[..., HEAD_DIM:], prior, cmp_value_in, cmp_value_out)
    cmp_piece = jnp.concatenate(
        [cmp_keys.astype(jnp.bfloat16), cmp_values.astype(jnp.bfloat16)], axis=-1
    )[:, None]
    picks = chosen[:, 0]
    every_list = lax.all_gather(picks[None, :, :, 1:], "kv", axis=0, tiled=True)
    named = jnp.any(every_list == place, axis=(0, 3)).astype(jnp.int32)
    seq_ids = jnp.arange(seqs, dtype=jnp.int32)[:, None]
    exported_seq = jnp.sum(named * seq_ids, axis=0)
    selector = seq_ids == exported_seq[None, :]
    export = jnp.sum(
        jnp.where(selector[:, None, :, None], sel_pairs, jnp.zeros((), jnp.bfloat16)), axis=0
    )
    export = export[None]
    remote_pairs, remote_entries = (
        lax.all_gather(export, "kv", axis=0, tiled=True),
        lax.all_gather(cmp_piece, "kv", axis=1, tiled=True),
    )
    gate_all = jnp.dot(rows, w_gate.reshape(width, 2 * HEADS), preferred_element_type=jnp.float32)
    gate_all = gate_all.reshape(seqs, span, 2, HEADS)
    gates = jax.nn.sigmoid(lax.dynamic_slice_in_dim(gate_all, column * local_heads, local_heads, 3))
    entry = jnp.arange(block_list * count, dtype=jnp.int32)
    entry_end = entry * CMP_STRIDE + CMP_STRIDE - 1
    cmp_valid = ((entry >= 1)[None, :] & (entry_end[None, :] <= positions[:, None]))[None, None]
    key_pos = jnp.arange(span, dtype=jnp.int32)
    own_valid = key_pos[None, :] <= key_pos[:, None]

    def one_sequence(args):
        seq_queries, seq_entries, seq_picks, seq_pairs, seq_gates, seq_length = args
        block_q = seq_queries.reshape(span, local_groups, per_group, HEAD_DIM)
        entries = seq_entries.reshape(block_list * count, local_groups, 2 * HEAD_DIM)
        scores = (
            jnp.einsum(
                "qghd,egd->ghqe",
                block_q,
                entries[..., :HEAD_DIM],
                preferred_element_type=jnp.float32,
            )
            * scale
        )
        weights = masked_weights(scores, cmp_valid)
        cmp_out = jnp.einsum(
            "ghqe,egd->qghd", weights, entries[..., HEAD_DIM:], preferred_element_type=jnp.float32
        )
        far = jnp.maximum(seq_picks[:, 1:], 0)
        fetched = jax.vmap(lambda table, index: table[index], in_axes=(2, 0))(remote_pairs, far)
        near = jnp.transpose(seq_pairs, (1, 0, 2))[:, None]
        pairs = jnp.concatenate([near, fetched], axis=1).reshape(
            local_groups, TOPK * span, 2 * HEAD_DIM
        )
        far_live = jnp.broadcast_to(
            (seq_picks[:, 1:] >= 0)[:, None, :, None], (local_groups, span, TOPK - 1, span)
        )
        near_live = jnp.broadcast_to(own_valid[None, :, None, :], (local_groups, span, 1, span))
        sel_valid = jnp.concatenate([near_live, far_live], axis=2).reshape(
            local_groups, 1, span, TOPK * span
        )
        scores_s = (
            jnp.einsum(
                "qghd,gmd->ghqm", block_q, pairs[..., :HEAD_DIM], preferred_element_type=jnp.float32
            )
            * scale
        )
        weights_s = masked_weights(scores_s, sel_valid)
        sel_out = jnp.einsum(
            "ghqm,gmd->qghd", weights_s, pairs[..., HEAD_DIM:], preferred_element_type=jnp.float32
        )
        split = seq_gates.reshape(span, 2, local_groups, per_group, 1)
        mixed = split[:, 0] * cmp_out + split[:, 1] * sel_out
        mixed = jnp.where((positions < seq_length)[:, None, None, None], mixed, 0.0)
        return mixed.reshape(span, local_heads * HEAD_DIM).astype(jnp.bfloat16)

    mixed = lax.map(one_sequence, (queries, remote_entries, picks, sel_pairs, gates, seq_lengths))
    mixed = mixed.reshape(seqs * span, local_heads * HEAD_DIM)
    out_width = width // lax.axis_size("tp")
    own_columns = lax.dynamic_slice_in_dim(w_out, column * out_width, out_width, 1)
    piece_wide = lax.all_gather(mixed, "tp", axis=1, tiled=True).astype(jnp.float32)
    scaled_piece = (piece_wide * out_gain[None, :]).astype(jnp.bfloat16)
    total = jnp.dot(scaled_piece, own_columns, preferred_element_type=jnp.float32)
    squares = jnp.sum(piece_wide * piece_wide, axis=-1)
    row_scale = lax.rsqrt(squares / (HEADS * HEAD_DIM) + norm_eps)
    return (total * row_scale[:, None]).astype(jnp.bfloat16).reshape(seqs, span, out_width)


FAR = -1e30
PLANE = 4
VMEM_BYTES = 60 * 1024 * 1024
f32 = jnp.float32
bf16 = jnp.bfloat16


def dot(a, b):
    return jnp.dot(a, b, preferred_element_type=f32)


def dot_t(a, b):
    return lax.dot_general(a, b, (((1,), (1,)), ((), ())), preferred_element_type=f32)


def turn(values, cosine, sine):
    lane = lax.broadcasted_iota(jnp.int32, values.shape, 1)
    other = jnp.where(
        lane % HEAD_DIM < HEAD_DIM // 2,
        pltpu.roll(values, 128 - HEAD_DIM // 2, 1),
        pltpu.roll(values, HEAD_DIM // 2, 1),
    )
    return values * cosine + other * sine


def gelu(x):
    return 0.5 * x * (1.0 + jnp.tanh(0.7978845608028654 * (x + 0.044715 * (x * x * x))))


def layer_kernel(
    n, seqs, span, heads,
    lens_ref, picks_ref, gain_ref, kout_ref, vout_ref,
    rows_ref, wq_ref, wck_ref, wcv_ref, wsk_ref, wsv_ref, wg_ref, kin_ref, vin_ref, wout_ref,
    out_ref,
    rows, wq, ws, wg, kin, vin, weight,
    q_buf, sk_buf, sv_buf, raw, gate_buf, lists, blobs, own, other, bias, near, partial,
    load_sem, pick_send, pick_recv, blob_send, blob_recv, half_send, half_recv,
):
    me = lax.axis_index("kv")
    column = lax.axis_index("tp")
    planes = n // PLANE
    z, x, c = me // PLANE, (me // 2) % 2, me % 2
    depth = heads * HEAD_DIM
    wide = out_ref.shape[1]
    count = span // CMP_STRIDE
    entries = seqs * count
    half = heads // 2
    mesh_id = pl.DeviceIdType.MESH

    pairs = [(rows_ref, rows)]
    for i, ref in enumerate((wsk_ref, wsv_ref, wck_ref, wcv_ref)):
        pairs.append((ref, ws.at[:, i * 128 : (i + 1) * 128]))
    pairs += [(kin_ref, kin), (vin_ref, vin), (wq_ref, wq), (wg_ref, wg)]
    for i in range(2):
        side = column if i == 0 else 1 - column
        block = wout_ref.at[
            pl.ds(pl.multiple_of(side * depth, depth), depth),
            pl.ds(pl.multiple_of(column * wide, wide), wide),
        ]
        pairs.append((block, weight.at[i]))
    loads = [pltpu.make_async_copy(a, b, load_sem.at[i]) for i, (a, b) in enumerate(pairs)]
    for load in loads:
        load.start()

    barrier = pltpu.get_barrier_semaphore()
    for d in range(1, n):
        pl.semaphore_signal(
            barrier, inc=1, device_id={"kv": (me + d) % n}, device_id_type=mesh_id
        )
    pl.semaphore_signal(barrier, inc=1, device_id={"tp": 1 - column}, device_id_type=mesh_id)

    lane = lax.broadcasted_iota(jnp.int32, (span, 128), 1)
    low = lane < HEAD_DIM
    low_e = low[:entries]
    at = lax.broadcasted_iota(jnp.int32, (span, 128), 0)
    sign = jnp.where(lane % HEAD_DIM < HEAD_DIM // 2, -1.0, 1.0)
    power = (lane % (HEAD_DIM // 2) * 2).astype(f32)
    freq = jnp.exp(-math.log(theta_base) * power / HEAD_DIM)
    angle = (me * span + at).astype(f32) * freq
    cosine = jnp.cos(angle)
    sine = jnp.sin(angle) * sign
    end = me * span + (at[:entries] % count) * CMP_STRIDE + CMP_STRIDE - 1
    angle = end.astype(f32) * freq[:entries]
    cosine_e = jnp.cos(angle)
    sine_e = jnp.sin(angle) * sign[:entries]
    row_q = lax.broadcasted_iota(jnp.int32, (span, span), 0)
    near[...] = jnp.where(
        lax.broadcasted_iota(jnp.int32, (span, span), 1) <= row_q, 0.0, FAR
    )
    far_keys = n * span
    block = lax.broadcasted_iota(jnp.int32, (2, far_keys), 1) // span
    for s in range(seqs):
        listed = picks_ref[s]
        hit = jnp.zeros((2, far_keys), jnp.int32)
        for j in range(1, TOPK):
            hit = jnp.where(block == listed[:, j : j + 1], 1, hit)
        bias[s] = jnp.where(hit > 0, 0.0, FAR)

    pl.semaphore_wait(barrier, n)
    sent = []
    for d in range(1, n):
        copy = pltpu.make_async_remote_copy(
            src_ref=picks_ref, dst_ref=lists.at[me], send_sem=pick_send.at[d - 1],
            recv_sem=pick_recv.at[me], device_id={"kv": (me + d) % n}, device_id_type=mesh_id,
        )
        copy.start()
        sent.append(copy)

    for load in loads[:5]:
        load.wait()
    made = dot(rows[...], ws[...])
    for s in range(seqs):
        part = slice(s * span, (s + 1) * span)
        sk_buf[part, :] = turn(made[part, :128], cosine, sine).astype(bf16)
    sv_buf[...] = made[:, 128:256].astype(bf16)
    raw[0] = made[:, 256:384].astype(bf16).astype(f32)
    raw[1] = made[:, 384:512].astype(bf16).astype(f32)
    first = at[:entries] % count == 0
    mid = CMP_STRIDE * HEAD_DIM
    for branch, inner_weight, outer in ((0, kin, kout_ref), (1, vin, vout_ref)):
        loads[5 + branch].wait()
        left, right = [], []
        for j in range(0, CMP_STRIDE, 2):
            a = raw[branch, pl.ds(j, entries, stride=CMP_STRIDE), :]
            b = raw[branch, pl.ds(j + 1, entries, stride=CMP_STRIDE), :]
            left.append(jnp.where(low_e, a, pltpu.roll(b, HEAD_DIM, 1)))
            right.append(jnp.where(low_e, pltpu.roll(a, HEAD_DIM, 1), b))
        window = jnp.concatenate(
            [jnp.concatenate(left, axis=1), jnp.concatenate(right, axis=1)], axis=0
        ).astype(bf16)
        front = dot(window, inner_weight[:mid])
        back = dot(window, inner_weight[mid:])
        parts = []
        for g in range(2):
            shifted = pltpu.roll(front[g * entries : (g + 1) * entries], 1, 0)
            parts.append(back[g * entries : (g + 1) * entries] + jnp.where(first, 0.0, shifted))
        inner = gelu(jnp.concatenate(parts, axis=0)).astype(bf16)
        outer = jnp.concatenate([outer[...], outer[...]], axis=0)
        result = dot_t(inner, outer)
        result = jnp.where(low_e, result[:entries], result[entries:])
        if branch == 0:
            result = turn(result, cosine_e, sine_e)
        start = 2 * span + branch * entries
        blobs[me, start : start + entries, :] = result.astype(bf16)

    named = jnp.zeros((seqs, 2, TOPK), jnp.int32)
    for d in range(1, n):
        origin = (me + d) % n
        pltpu.make_async_remote_copy(
            src_ref=picks_ref, dst_ref=lists.at[origin], send_sem=pick_send.at[d - 1],
            recv_sem=pick_recv.at[origin], device_id={"kv": origin}, device_id_type=mesh_id,
        ).wait_recv()
        named = jnp.maximum(named, (lists[origin] == me).astype(jnp.int32))
    slot_at = lax.broadcasted_iota(jnp.int32, (seqs, 2, TOPK), 2)
    named = jnp.max(jnp.where(slot_at == 0, 0, named), axis=2, keepdims=True)
    key = jnp.zeros((span, 128), f32)
    value = jnp.zeros((span, 128), f32)
    for s in range(seqs):
        flag = jnp.where(low, named[s, 0:1, :], named[s, 1:2, :]) > 0
        key = jnp.where(flag, sk_buf[s * span : (s + 1) * span, :].astype(f32), key)
        value = jnp.where(flag, sv_buf[s * span : (s + 1) * span, :].astype(f32), value)
    blobs[me, 0:span, :] = key.astype(bf16)
    blobs[me, span : 2 * span, :] = value.astype(bf16)

    def pass_on(slot, dst, number):
        copy = pltpu.make_async_remote_copy(
            src_ref=blobs.at[slot], dst_ref=blobs.at[slot], send_sem=blob_send.at[number],
            recv_sem=blob_recv.at[slot], device_id={"kv": dst}, device_id_type=mesh_id,
        )
        copy.start()
        sent.append(copy)

    def arrived(slot):
        pltpu.make_async_remote_copy(
            src_ref=blobs.at[slot], dst_ref=blobs.at[slot], send_sem=blob_send.at[0],
            recv_sem=blob_recv.at[slot], device_id={"kv": (me + 1) % n}, device_id_type=mesh_id,
        ).wait_recv()

    across = z * PLANE + (1 - x) * 2 + c
    beside = z * PLANE + x * 2 + (1 - c)
    order = sorted(range(1, planes), key=lambda d: (min(d, planes - d), d))
    number = 0
    for d in order:
        pass_on(me, ((z + d) % planes) * PLANE + x * 2 + c, number)
        number += 1
    pass_on(me, across, number)
    pass_on(me, beside, number + 1)
    number += 2

    loads[7].wait()
    loads[8].wait()
    hidden = rows[...]
    for i in range(half):
        made = dot(hidden, wq[:, i * 128 : (i + 1) * 128])
        for s in range(seqs):
            v = turn(made[s * span : (s + 1) * span], cosine, sine) * (HEAD_DIM**-0.5)
            y = pltpu.roll(v, HEAD_DIM, 1)
            if 2 * i < half:
                even, odd = jnp.where(low, v, 0.0), jnp.where(low, y, 0.0)
            else:
                even, odd = jnp.where(low, 0.0, y), jnp.where(low, 0.0, v)
            base = (s * heads + 2 * i) * span
            q_buf[base : base + span, :] = even.astype(bf16)
            q_buf[base + span : base + 2 * span, :] = odd.astype(bf16)
    spread = 2 * wg_ref.shape[1]
    gate_buf[...] = jnp.zeros_like(gate_buf)
    gate_buf[:, :spread] = jax.nn.sigmoid(dot_t(hidden, wg[...].reshape(spread, rows.shape[1])))

    for d in order:
        slot = ((z + planes - d) % planes) * PLANE + x * 2 + c
        arrived(slot)
        pass_on(slot, across, number)
        pass_on(slot, beside, number + 1)
        number += 2
    for d in [0] + order:
        slot = ((z + planes - d) % planes) * PLANE + (1 - x) * 2 + c
        arrived(slot)
        pass_on(slot, beside, number)
        number += 1
    for d in [0] + order:
        origin = ((z + planes - d) % planes) * PLANE
        arrived(origin + x * 2 + (1 - c))
        arrived(origin + (1 - x) * 2 + (1 - c))

    slot = lax.broadcasted_iota(jnp.int32, (span, n * entries), 1)
    entry = (slot // entries) * count + slot % count
    entry_seq = (slot % entries) // count
    query_at = me * span + lax.broadcasted_iota(jnp.int32, (span, n * entries), 0)
    entry_ok = (entry >= 1) & (entry * CMP_STRIDE + CMP_STRIDE - 1 <= query_at)
    row_at = me * span + at
    far_k = blobs[:, 0:span, :].reshape(far_keys, 128)
    far_v = blobs[:, span : 2 * span, :].reshape(far_keys, 128)
    cmp_k = blobs[:, 2 * span : 2 * span + entries, :].reshape(n * entries, 128)
    cmp_v = blobs[:, 2 * span + entries :, :].reshape(n * entries, 128)

    def piece(s):
        return pltpu.make_async_remote_copy(
            src_ref=own.at[s], dst_ref=other.at[s], send_sem=half_send.at[s],
            recv_sem=half_recv.at[s], device_id={"tp": 1 - column}, device_id_type=mesh_id,
        )

    def one_sequence(s, carry):
        part = pl.ds(pl.multiple_of(s * span, span), span)
        near_k = sk_buf[part, :]
        near_v = sv_buf[part, :]
        gates = gate_buf[part, :]
        gates = jnp.where(column == 0, gates, pltpu.roll(gates, 128 - heads, 1))
        live = row_at < lens_ref[s]
        entry_bias = jnp.where(entry_ok & (entry_seq == s), 0.0, FAR)
        for g in range(2):
            start = pl.multiple_of((s * heads + g * half) * span, span)
            q = q_buf[pl.ds(start, half * span), :]
            sc = dot_t(q, cmp_k).reshape(half, span, n * entries) + entry_bias[None]
            top = jnp.maximum(jnp.max(sc, axis=-1, keepdims=True), -1e29)
            e = jnp.exp(sc - top)
            total = jnp.maximum(jnp.sum(e, axis=-1, keepdims=True), 1.0)
            w = (e * (1.0 / total)).astype(bf16).reshape(half * span, n * entries)
            cmp_out = dot(w, cmp_v)
            sf = dot_t(q, far_k) + bias[s, g : g + 1, :]
            sn = (dot_t(q, near_k).reshape(half, span, span) + near[...][None]).reshape(
                half * span, span
            )
            top = jnp.maximum(
                jnp.max(sf, axis=-1, keepdims=True), jnp.max(sn, axis=-1, keepdims=True)
            )
            ef = jnp.exp(sf - top)
            en = jnp.exp(sn - top)
            total = jnp.sum(ef, axis=-1, keepdims=True) + jnp.sum(en, axis=-1, keepdims=True)
            inverse = 1.0 / total
            sel_out = dot((ef * inverse).astype(bf16), far_v) + dot(
                (en * inverse).astype(bf16), near_v
            )
            mixed = []
            for h in range(half):
                span_h = slice(h * span, (h + 1) * span)
                head = g * half + h
                behind = spread // 2 + head
                mixed.append(
                    gates[:, head : head + 1] * cmp_out[span_h]
                    + gates[:, behind : behind + 1] * sel_out[span_h]
                )
            for h in range(0, half, 2):
                if g == 0:
                    pair = jnp.where(low, mixed[h], pltpu.roll(mixed[h + 1], HEAD_DIM, 1))
                else:
                    pair = jnp.where(low, pltpu.roll(mixed[h], HEAD_DIM, 1), mixed[h + 1])
                pair = jnp.where(live, pair, 0.0).astype(bf16)
                lanes = (g * half + h) * HEAD_DIM
                own[s, :, lanes : lanes + 128] = pair
        piece(s).start()
        return carry

    lax.fori_loop(0, seqs, one_sequence, 0)
    for load in loads[9:]:
        load.wait()
    gain_own = gain_ref[:, pl.ds(pl.multiple_of(column * depth, depth), depth)]
    gain_other = gain_ref[:, pl.ds(pl.multiple_of((1 - column) * depth, depth), depth)]

    def begin(s, carry):
        partial[s] = dot((own[s].astype(f32) * gain_own).astype(bf16), weight[0])
        return carry

    lax.fori_loop(0, seqs, begin, 0)

    def finish(s, carry):
        piece(s).wait_recv()
        a = own[s].astype(f32)
        b = other[s].astype(f32)
        squares = jnp.sum(a * a, axis=-1, keepdims=True) + jnp.sum(b * b, axis=-1, keepdims=True)
        row_scale = lax.rsqrt(squares / (2 * depth) + norm_eps)
        total = partial[s] + dot((b * gain_other).astype(bf16), weight[1])
        out_ref[pl.ds(pl.multiple_of(s * span, span), span), :] = (total * row_scale).astype(bf16)
        return carry

    lax.fori_loop(0, seqs, finish, 0)

    def close(s, carry):
        piece(s).wait_send()
        return carry

    lax.fori_loop(0, seqs, close, 0)
    for copy in sent:
        copy.wait_send()


def fused_shards(
    hidden_in,
    w_query,
    w_cmp_key,
    w_cmp_value,
    w_sel_key,
    w_sel_value,
    w_gate,
    cmp_key_in,
    cmp_key_out,
    cmp_value_in,
    cmp_value_out,
    out_gain,
    w_out,
    seq_lengths,
    chosen,
):
    seqs, span, width = hidden_in.shape
    n = lax.axis_size("kv")
    heads = w_query.shape[1] // HEAD_DIM
    total = seqs * span
    entries = total // CMP_STRIDE
    out_width = width // lax.axis_size("tp")
    small = w_sel_key.shape[1]
    vmem = pl.BlockSpec(memory_space=pltpu.VMEM)
    anywhere = pl.BlockSpec(memory_space=pl.ANY)
    gate_rows = jnp.transpose(w_gate, (1, 2, 0))
    out = pl.pallas_call(
        functools.partial(layer_kernel, n, seqs, span, heads),
        in_specs=[pl.BlockSpec(memory_space=pltpu.SMEM)] + [vmem] * 4 + [anywhere] * 10,
        out_specs=vmem,
        out_shape=jax.ShapeDtypeStruct((total, out_width), bf16),
        scratch_shapes=[
            pltpu.VMEM((total, width), bf16),
            pltpu.VMEM(w_query.shape, bf16),
            pltpu.VMEM((width, 4 * small), bf16),
            pltpu.VMEM(gate_rows.shape, bf16),
            pltpu.VMEM(cmp_key_in.shape, bf16),
            pltpu.VMEM(cmp_value_in.shape, bf16),
            pltpu.VMEM((2, heads * HEAD_DIM, out_width), bf16),
            pltpu.VMEM((heads * total, 128), bf16),
            pltpu.VMEM((total, small), bf16),
            pltpu.VMEM((total, small), bf16),
            pltpu.VMEM((2, total, small), f32),
            pltpu.VMEM((total, 128), f32),
            pltpu.VMEM((n, seqs, 2, TOPK), jnp.int32),
            pltpu.VMEM((n, 2 * span + 2 * entries, small), bf16),
            pltpu.VMEM((seqs, span, heads * HEAD_DIM), bf16),
            pltpu.VMEM((seqs, span, heads * HEAD_DIM), bf16),
            pltpu.VMEM((seqs, 2, n * span), f32),
            pltpu.VMEM((span, span), f32),
            pltpu.VMEM((seqs, span, out_width), f32),
            pltpu.SemaphoreType.DMA((11,)),
            pltpu.SemaphoreType.DMA((n,)),
            pltpu.SemaphoreType.DMA((n,)),
            pltpu.SemaphoreType.DMA((n,)),
            pltpu.SemaphoreType.DMA((n,)),
            pltpu.SemaphoreType.DMA((seqs,)),
            pltpu.SemaphoreType.DMA((seqs,)),
        ],
        compiler_params=pltpu.CompilerParams(
            collective_id=0, has_side_effects=True, vmem_limit_bytes=VMEM_BYTES
        ),
        name="layer",
    )(
        seq_lengths, chosen[:, 0], out_gain[None],
        jnp.transpose(cmp_key_out), jnp.transpose(cmp_value_out),
        hidden_in.reshape(total, width), w_query, w_cmp_key, w_cmp_value, w_sel_key,
        w_sel_value, gate_rows, cmp_key_in, cmp_value_in, w_out,
    )
    return out.reshape(seqs, span, out_width)


def fits(mesh):
    n = mesh.shape["kv"]
    return mesh.shape["tp"] == 2 and n % PLANE == 0 and n <= 32


def solution(mesh):
    placed = (
        P(None, "kv", None),
        P(None, "tp"),
        P(None, "tp"),
        P(None, "tp"),
        P(None, "tp"),
        P(None, "tp"),
        P(),
        P(),
        P(),
        P(),
        P(),
        P(),
        P(),
        P(),
        P(None, "kv", "tp", None),
    )
    return jax.shard_map(
        fused_shards if fits(mesh) else shards, mesh=mesh, in_specs=placed, out_specs=P(None, "kv", "tp"), check_vma=False
    )
```
